256 devices in a mesh: grp: 2 (over y), fs: 16 (over z), tp: 8 (over x, core).
Axes of the slice: x: 4, y: 2, z: 16, core: 2. Of those that a mesh axis runs over, the one named last changes fastest.
The devices are a block of a 4x16x16 slice.
Arguments:
- tokens: bfloat16 [32, 1024, 2048], P(('grp', 'fs'), None, 'tp'), parts along dimension 0, may hold values from -6 to 6
- mix_gain: float32 [2048], replicated, may hold values from 0.1 to 1.9
- in_matrix: float32 [2048, 1024], P('fs', 'tp'), may hold values from -0.125 to 0.125
- in_scale: float32 [1, 1024], P(None, 'tp'), may hold values from 0.5 to 2
- pool_mix: bfloat16 [8, 128, 128], P('tp'), may hold values from -0.5 to 0.5
- pool_scale: float32 [1, 1024], P(None, 'tp'), may hold values from 0.1 to 1.9
- out_matrix: float32 [1024, 2048], P('tp', 'fs'), may hold values from -0.25 to 0.25
- out_scale: float32 [1, 2048], P(None, 'fs'), may hold values from 0.5 to 2
- ffn_gain: float32 [2048], replicated, may hold values from 0.1 to 1.9
- gate_matrix: float32 [2048, 5632], P('fs', 'tp'), may hold values from -0.125 to 0.125
- gate_scale: float32 [1, 5632], P(None, 'tp'), may hold values from 0.5 to 2
- up_matrix: float32 [2048, 5632], P('fs', 'tp'), may hold values from -0.125 to 0.125
- up_scale: float32 [1, 5632], P(None, 'tp'), may hold values from 0.5 to 2
- gate_taps: float32 [3, 5632], P(None, 'tp'), may hold values from -4 to 4
- up_taps: float32 [3, 5632], P(None, 'tp'), may hold values from -4 to 4
- down_matrix: float32 [5632, 2048], P('tp', 'fs'), may hold values from -0.109375 to 0.109375
- down_scale: float32 [1, 2048], P(None, 'fs'), may hold values from 0.5 to 2
Outputs:
- layer_out: bfloat16 [32, 1024, 2048], P(('grp', 'fs'), None, 'tp'), parts along dimension 0
The draws below stay inside these ranges and needn't reach their ends.
There are 2 independent parts, one for each index of `grp`. The reference program is written for one: setup_inputs(seed, part) draws one part's arguments, and reference() takes and returns one part's arrays. A program takes and returns all parts, laid end to end along the dimension named above; an argument that names none is the same for every part. Nothing has to cross between parts.
All inputs are finite; a program needn't handle non-finite values.
Results may differ from the reference program's by a relative error of at most 0.025.
Values may be sent and summed in bfloat16 or wider, within the bound.
A program may use at most 64 MiB of HBM per device.

```python
import math
import jax
import jax.numpy as jnp
from jax import lax

D = 2048
BLOCKS = 8
BLOCK_CH = 128
FF = 5632
LEN = 1024
PW = 1024
SEQS = 16
COL_GROUPS = 8


def raised(array, stream_key, source, target, shards_of, factor):
    def block_of(dim):
        return (jnp.arange(array.shape[dim]) // (array.shape[dim] // shards_of)).reshape((-1,) + (1,) * (array.ndim - 1 - dim))

    near = jax.random.permutation(stream_key, shards_of)[block_of(target)]
    far = (block_of(target) + shards_of // 2) % shards_of
    return jnp.where((block_of(source) == near) | (block_of(source) == far), factor * array, array)


def levels(stream_key, shape, pieces, least, top_value):
    level, own = 1.0, jax.random.fold_in(stream_key, 6)
    for dim, shards_of in pieces:
        steps = jnp.exp(jax.random.uniform(jax.random.fold_in(own, dim), (shards_of,), jnp.float32, least / len(pieces), top_value / len(pieces)))
        level = level * jnp.repeat(steps, shape[dim] // shards_of).reshape([-1 if axis == dim else 1 for axis in range(len(shape))])
    return level


def bell_draw(own_key, shape, deviation, reach, pieces=(), kind=jnp.bfloat16):
    drawn = deviation * jax.random.normal(own_key, shape, jnp.float32)
    if pieces:
        drawn = drawn * levels(own_key, shape, pieces, -0.22, 0.18)
    return jnp.clip(drawn, -reach, reach).astype(kind)


def gaussian_with(rng, shape, width, reach, cuts, heavy, held_as=jnp.bfloat16):
    drawn = width * jax.random.normal(rng, shape, jnp.float32)
    if cuts:
        drawn = drawn * levels(rng, shape, cuts, -0.22, 0.18)
    return jnp.clip(raised(drawn, jax.random.fold_in(rng, 3), *heavy), -reach, reach).astype(held_as)


def setup_inputs(seed: int = 0, part: int = 0) -> dict:
    streams_of = jax.random.split(jax.random.key(seed), 18)
    part_keys = jax.random.split(jax.random.fold_in(streams_of[17], part), 18)
    tokens = bell_draw(part_keys[0], (SEQS, LEN, D), 1.0, 6.0, ((0, 16), (2, 8)))
    mix_gain = jnp.clip(1.0 + 0.18 * jax.random.normal(streams_of[1], (D,), jnp.float32), 0.1, 1.9)
    in_matrix = bell_draw(streams_of[2], (D, PW), D ** -0.5, 0.125, ((0, 16), (1, 8)), jnp.float32)
    in_scale = jnp.clip(jnp.exp(math.log(2.0) - 1.3862944 * jax.random.uniform(streams_of[3], (1, PW), jnp.float32) ** levels(streams_of[3], (1, PW), ((1, 8),), -0.2, 0.2)), 0.5, 2.0)
    pool_mix = bell_draw(streams_of[4], (BLOCKS, BLOCK_CH, BLOCK_CH), BLOCK_CH ** -0.5, 0.5, ((0, 8),))
    pool_scale = jnp.clip(1.0 + 0.18 * jax.random.normal(streams_of[5], (1, PW), jnp.float32), 0.1, 1.9)
    out_matrix = gaussian_with(streams_of[6], (PW, D), PW ** -0.5, 0.25, ((0, 8), (1, 16)), (0, 1, 16, 2.0), jnp.float32)
    out_scale = jnp.clip(jnp.exp(math.log(2.0) - 1.3862944 * jax.random.uniform(streams_of[7], (1, D), jnp.float32) ** levels(streams_of[7], (1, D), ((1, 16),), -0.2, 0.2)), 0.5, 2.0)
    ffn_gain = jnp.clip(1.0 + 0.18 * jax.random.normal(streams_of[8], (D,), jnp.float32), 0.1, 1.9)
    gate_matrix = bell_draw(streams_of[9], (D, FF), D ** -0.5, 0.125, ((0, 16), (1, 8)), jnp.float32)
    gate_scale = jnp.clip(jnp.exp(math.log(2.0) - 1.3862944 * jax.random.uniform(streams_of[10], (1, FF), jnp.float32) ** levels(streams_of[10], (1, FF), ((1, 8),), -0.2, 0.2)), 0.5, 2.0)
    up_matrix = bell_draw(streams_of[11], (D, FF), D ** -0.5, 0.125, ((0, 16), (1, 8)), jnp.float32)
    up_scale = jnp.clip(jnp.exp(math.log(2.0) - 1.3862944 * jax.random.uniform(streams_of[12], (1, FF), jnp.float32) ** levels(streams_of[12], (1, FF), ((1, 8),), -0.2, 0.2)), 0.5, 2.0)
    gate_taps = bell_draw(streams_of[13], (3, FF), 0.58, 4.0, ((1, 8),), jnp.float32)
    up_taps = bell_draw(streams_of[14], (3, FF), 0.58, 4.0, ((1, 8),), jnp.float32)
    down_matrix = gaussian_with(streams_of[15], (FF, D), FF ** -0.5, 0.109375, ((0, 8), (1, 16)), (0, 1, 16, 2.0), jnp.float32)
    down_scale = jnp.clip(jnp.exp(math.log(2.0) - 1.3862944 * jax.random.uniform(streams_of[16], (1, D), jnp.float32) ** levels(streams_of[16], (1, D), ((1, 16),), -0.2, 0.2)), 0.5, 2.0)
    return {"tokens": tokens, "mix_gain": mix_gain, "in_matrix": in_matrix, "in_scale": in_scale, "pool_mix": pool_mix, "pool_scale": pool_scale, "out_matrix": out_matrix, "out_scale": out_scale, "ffn_gain": ffn_gain, "gate_matrix": gate_matrix, "gate_scale": gate_scale, "up_matrix": up_matrix, "up_scale": up_scale, "gate_taps": gate_taps, "up_taps": up_taps, "down_matrix": down_matrix, "down_scale": down_scale}


eps = 1e-06
widest_span = 16

def norm_rows(tok_rows, norm_gain):
    values = tok_rows.astype(jnp.float32)
    scaled = values * lax.rsqrt(lax.optimization_barrier(jnp.mean(values * values, axis=-1, keepdims=True)) + eps)
    return (scaled * norm_gain.astype(jnp.float32)).astype(jnp.bfloat16)

def span_widths(block_ids):
    return jnp.left_shift(jnp.ones_like(block_ids), (1 + 4 * block_ids // BLOCKS).astype(jnp.int32))

def trailing_gap(projected, windows):
    values = projected.astype(jnp.float32)
    length = values.shape[0]
    running = values
    for offset in range(1, widest_span):
        shifted = jnp.pad(values[:length - offset], ((offset, 0), (0, 0)))
        running = running + jnp.where(windows[None, :] > offset, shifted, jnp.zeros_like(shifted))
    positions = jnp.arange(length, dtype=jnp.int32)[:, None]
    counts = jnp.minimum(positions + 1, windows[None, :]).astype(jnp.float32)
    return (running / counts - values).astype(jnp.bfloat16)

def causal_taps(linear, tap_table):
    values = linear.astype(jnp.float32)
    length = values.shape[0]
    back_one = jnp.pad(values[:length - 1], ((1, 0), (0, 0)))
    back_two = jnp.pad(values[:length - 2], ((2, 0), (0, 0)))
    return tap_table[2] * values + tap_table[1] * back_one + tap_table[0] * back_two

def grouped_product(operand, matrix, scales):
    narrow = operand.shape[1] // COL_GROUPS
    cast_matrix = matrix.astype(jnp.bfloat16)
    running = jnp.zeros((operand.shape[0], matrix.shape[1]), jnp.float32)
    for member in range(COL_GROUPS):
        partial_value = jnp.dot(operand[:, member * narrow:(member + 1) * narrow], cast_matrix[member * narrow:(member + 1) * narrow], preferred_element_type=jnp.float32) * scales
        rounded = lax.optimization_barrier(partial_value.astype(jnp.bfloat16))
        running = running + rounded.astype(jnp.float32)
    return running

def reference(tokens, mix_gain, in_matrix, in_scale, pool_mix, pool_scale, out_matrix, out_scale, ffn_gain, gate_matrix, gate_scale, up_matrix, up_scale, gate_taps, up_taps, down_matrix, down_scale):
    windows = jnp.repeat(span_widths(jnp.arange(BLOCKS, dtype=jnp.int32)), BLOCK_CH)
    in_cast = in_matrix.astype(jnp.bfloat16)
    gate_cast = gate_matrix.astype(jnp.bfloat16)
    up_cast = up_matrix.astype(jnp.bfloat16)

    def single(sequence):
        normed = norm_rows(sequence, mix_gain)
        projected = (jnp.dot(normed, in_cast, preferred_element_type=jnp.float32) * in_scale).astype(jnp.bfloat16)
        spread = trailing_gap(projected, windows)
        blocks = spread.reshape(-1, BLOCKS, BLOCK_CH).astype(jnp.float32)
        block_mixed = jnp.einsum('lbc,bce->lbe', blocks, pool_mix.astype(jnp.float32)).reshape(-1, PW)
        pooled = (block_mixed * pool_scale).astype(jnp.bfloat16)
        mixing = grouped_product(pooled, out_matrix, out_scale)
        residual = (sequence.astype(jnp.float32) + mixing).astype(jnp.bfloat16)
        normed_ffn = norm_rows(residual, ffn_gain)
        gate_lin = (jnp.dot(normed_ffn, gate_cast, preferred_element_type=jnp.float32) * gate_scale).astype(jnp.bfloat16)
        up_lin = (jnp.dot(normed_ffn, up_cast, preferred_element_type=jnp.float32) * up_scale).astype(jnp.bfloat16)
        hidden = (jax.nn.silu(causal_taps(gate_lin, gate_taps)) * causal_taps(up_lin, up_taps)).astype(jnp.bfloat16)
        feed_out = grouped_product(hidden, down_matrix, down_scale)
        return (residual.astype(jnp.float32) + feed_out).astype(jnp.bfloat16)
    return lax.map(single, tokens)
```

```python
import functools

import jax
import jax.numpy as jnp
from jax import lax
from jax.experimental import pallas as pl
from jax.experimental.pallas import tpu as pltpu
from jax.sharding import PartitionSpec as P

MESH = pl.DeviceIdType.MESH
EPS = 1e-06
BF16 = jnp.bfloat16
F32 = jnp.float32
LANES = 128
CORES = 2


class FeatureGather:
    TAGS = 13
    R0, R1, L1, L0, F0, F1, OWN, PL0, PL1, PR0, PR1, PO0, PO1 = range(13)

    def __init__(self, buf, send, recv, chips, x, core):
        self.buf, self.send, self.recv = buf, send, recv
        self.half = buf.shape[1] // 2
        at = lambda chip, c: lax.rem(chip, chips) * CORES + c
        other = 1 - core
        self.me, self.mate = at(x, core), at(x, other)
        self.right, self.left, self.far = at(x + 1, core), at(x + chips - 1, core), at(x + 2, core)
        mright, mleft, mfar = at(x + 1, other), at(x + chips - 1, other), at(x + 2, other)
        self.out = {
            self.R0: (self.me, 0, self.right), self.R1: (self.me, 1, self.right),
            self.L1: (self.me, 1, self.left), self.L0: (self.me, 0, self.left),
            self.F0: (self.left, 0, self.right), self.F1: (self.right, 1, self.left),
            self.OWN: (self.me, None, self.mate),
            self.PL0: (self.left, 0, self.mate), self.PL1: (self.left, 1, self.mate),
            self.PR0: (self.right, 0, self.mate), self.PR1: (self.right, 1, self.mate),
            self.PO0: (self.far, 0, self.mate), self.PO1: (self.far, 1, self.mate),
        }
        self.inn = {
            self.R0: (self.left, 0), self.R1: (self.left, 1),
            self.L1: (self.right, 1), self.L0: (self.right, 0),
            self.F0: (self.far, 0), self.F1: (self.far, 1),
            self.OWN: (self.mate, None),
            self.PL0: (mleft, 0), self.PL1: (mleft, 1),
            self.PR0: (mright, 0), self.PR1: (mright, 1),
            self.PO0: (mfar, 0), self.PO1: (mfar, 1),
        }
        self.then = {
            self.R0: (self.F0, self.PL0), self.L1: (self.F1, self.PR1),
            self.R1: (self.PL1,), self.L0: (self.PR0,),
            self.F0: (self.PO0,), self.F1: (self.PO1,),
        }

    def ref(self, block, part):
        if part is None:
            return self.buf.at[block]
        return self.buf.at[block, pl.ds(part * self.half, self.half)]

    def copy(self, tag, block, part, to):
        ref = self.ref(block, part)
        return pltpu.make_async_remote_copy(
            ref, ref, self.send.at[tag], self.recv.at[tag], device_id={"tp": to}, device_id_type=MESH
        )

    def start(self):
        for tag in (self.R0, self.L1, self.R1, self.L0, self.OWN):
            self.copy(tag, *self.out[tag]).start()

    def arrive(self, *tags):
        for tag in tags:
            self.copy(tag, *self.inn[tag], self.mate).wait_recv()
            for later in self.then.get(tag, ()):
                self.copy(later, *self.out[later]).start()

    def finish(self):
        self.arrive(self.OWN, self.PL0, self.PR1, self.PL1, self.PR0, self.PO0, self.PO1)

    def drain(self):
        for tag in range(self.TAGS):
            self.copy(tag, *self.out[tag]).wait_send()


def kernel(
    zn, tn,
    tok_in, mix_gain, in_m, in_s, pool_m, pool_s, out_m, out_s, ffn_gain,
    gate_m, gate_s, up_m, up_s, gate_t, up_t, down_m, down_s,
    out_ref,
    tok, res, nf, io, inw, outg, outw, proj, pool, gu, par, lin, hid, dn, sbuf, rsb,
    load_sem, zsend, zrecv, gsend, grecv, osend, orecv, hsend, hrecv, dsend, drecv, rsend, rrecv,
):
    z, me = lax.axis_index("fs"), lax.axis_index("tp")
    x, core = lax.div(me, CORES), lax.rem(me, CORES)
    other = 1 - core
    mate = x * CORES + other
    chips = tn // CORES
    zright, zleft = lax.rem(z + 1, zn), lax.rem(z + zn - 1, zn)
    hops = zn // 2

    length, width = tok_in.shape
    depth, chan = in_m.shape
    ff = gate_m.shape[1]
    ocols = out_m.shape[1]
    full = ff // LANES
    tail = ff - full * LANES
    per = width // ocols

    load = pltpu.make_async_copy(tok_in, tok.at[me], load_sem)
    load.start()

    io[z, 0:depth, :] = in_m[...].astype(BF16)
    io[z, depth:, :] = (out_m[...] * out_s[...]).astype(BF16)

    def packed(g_ref, u_ref):
        for j in range(full):
            cols = slice(j * LANES, (j + 1) * LANES)
            yield 2 * j * LANES, jnp.concatenate([g_ref[:, cols], u_ref[:, cols]], axis=1)
        yield 2 * full * LANES, jnp.concatenate([g_ref[:, full * LANES :], u_ref[:, full * LANES :]], axis=1)

    own_rows = pl.ds(pl.multiple_of(z * depth, depth), depth)
    for at, v in packed(gate_m, up_m):
        gu[own_rows, at : at + v.shape[1]] = v.astype(BF16)
    for at, v in packed(gate_s, up_s):
        par[0:1, at : at + v.shape[1]] = v
    for at, v in packed(gate_t, up_t):
        par[1:4, at : at + v.shape[1]] = v
    dn[core, z, 0:ff, :] = (down_m[...] * down_s[...]).astype(BF16)
    dpad = dn.shape[2]

    def clear(i, _):
        dn[0, i, ff:dpad, :] = jnp.zeros((dpad - ff, ocols), BF16)
        dn[1, i, ff:dpad, :] = jnp.zeros((dpad - ff, ocols), BF16)
        return 0

    lax.fori_loop(0, zn, clear, 0)
    lin[0:8, :] = jnp.zeros((8, lin.shape[1]), F32)
    load.wait()

    barrier = pltpu.get_barrier_semaphore()
    for to in (zleft, zright):
        pl.semaphore_signal(barrier, inc=1, device_id={"fs": to}, device_id_type=MESH)
    for j in range(1, tn):
        pl.semaphore_signal(barrier, inc=1, device_id={"tp": lax.rem(me + j, tn)}, device_id_type=MESH)
    pl.semaphore_wait(barrier, tn + 1)

    def io_part(slot, part):
        n = 2 * depth
        if part is None:
            return io.at[slot]
        return io.at[slot, pl.ds(part * (n // 2), n // 2)]

    def gu_part(r0, n, first):
        def at(slot, part):
            a, m = ((r0, n), (r0, first), (r0 + first, n - first))[0 if part is None else part + 1]
            return gu.at[pl.ds(pl.multiple_of(slot * depth + a, 16), m)]

        return at

    def dn_part(r0, n):
        def at(slot, part):
            a, m = (r0, n) if part is None else (r0 + part * (n // 2), n // 2)
            return dn.at[core, slot, pl.ds(a, m)]

        return at

    q = depth // 8
    lanes = [
        io_part,
        gu_part(0, 2 * q, q),
        gu_part(2 * q, 3 * q, 2 * q),
        gu_part(5 * q, 3 * q, 2 * q),
        dn_part(0, ff // 2),
        dn_part(ff // 2, ff // 2),
    ]
    A, B0, B1, B2, C1, C2 = range(6)

    def zslot(d, s):
        return lax.rem(z + zn + (s if d else -s), zn)

    def zcopy(i, d, s, part, slot):
        ref = lanes[i](slot, part)
        return pltpu.make_async_remote_copy(
            ref, ref, zsend.at[i, d], zrecv.at[i, d, s - 1],
            device_id={"fs": zleft if d else zright}, device_id_type=MESH,
        )

    def zput(i, d, s, part=None):
        return zcopy(i, d, s, part, zslot(d, s - 1))

    def zgot(i, d, s, part=None):
        zcopy(i, d, s, part, zslot(d, s)).wait_recv()

    def zopen(i):
        for d in range(2):
            zput(i, d, 1).start()

    def tick(i, s):
        for d in range(2):
            static = isinstance(s, int)
            part = d if static and s == hops else None
            zgot(i, d, s, part)
            zput(i, d, s, part).wait_send()
            if not static or s < hops - 1:
                zput(i, d, s + 1).start()
            elif s == hops - 1:
                zput(i, d, s + 1, d).start()

    def steps():
        for s in range(1, hops + 1):
            tick(A, s)
            if s == hops - 1:
                zopen(B1)
            yield
            tick(B0, s)
            if s == hops - 1:
                zopen(B2)
            yield
        for s in range(1, hops + 1):
            tick(B1, s)
            if s == hops - 1:
                zopen(C1)
            yield
            tick(B2, s)
            if s == hops - 1:
                zopen(C2)
            yield

    ring = steps()

    def go(n):
        for _ in range(n):
            next(ring)

    gathers = [
        FeatureGather(buf, gsend.at[k], grecv.at[k], chips, x, core) for k, buf in enumerate((tok, pool, res))
    ]
    g_tok, g_pool, g_res = gathers
    G = FeatureGather

    def hand(d, s, which, slot):
        ref = dn.at[which, slot, pl.ds(0, ff)]
        return pltpu.make_async_remote_copy(
            ref, ref, dsend.at[d, s], drecv.at[d, s], device_id={"tp": mate}, device_id_type=MESH
        )

    zopen(A)
    zopen(B0)
    g_tok.start()
    hand(0, 0, core, z).start()

    def norm(buf, gain_ref, lo, hi):
        rows = 32

        def body(i, _):
            r = pl.ds(pl.multiple_of(i * rows, rows), rows)
            total = jnp.zeros((rows, width), F32)
            for p in range(tn):
                v = buf[p, r, :].astype(F32)
                total = total + v * v
            mean = jnp.sum(total, axis=1, keepdims=True) * (1.0 / (tn * width))
            scale = lax.rsqrt(mean + EPS)
            for p in range(tn):
                cols = slice(p * width, (p + 1) * width)
                nf[r, cols] = (buf[p, r, :].astype(F32) * scale * gain_ref[:, cols]).astype(BF16)
            return 0

        lax.fori_loop(lo // rows, hi // rows, body, 0)

    go(2)
    g_tok.arrive(G.R0, G.L1)
    go(4)
    g_tok.arrive(G.R1, G.L0)
    go(2)
    g_tok.arrive(G.F0, G.F1)
    go(2)
    g_tok.finish()
    norm(tok, mix_gain, 0, length // 2)
    go(2)
    norm(tok, mix_gain, length // 2, length)
    go(4)

    def own_rows_copy(j, block, to):
        return pltpu.make_async_remote_copy(
            io.at[pl.ds(to * per, per), pl.ds(depth, depth)], outg.at[block],
            osend.at[j], orecv.at[j], device_id={"tp": to}, device_id_type=MESH,
        )

    for j in range(1, tn):
        own_rows_copy(j, me, lax.rem(me + j, tn)).start()
    outg[me] = io[pl.ds(me * per, per), depth:, :]

    for k in range(zn):
        inw[k * depth : (k + 1) * depth, :] = io[k, 0:depth, :]
    tile = length // 4

    def project(i, _):
        r = pl.ds(pl.multiple_of(i * tile, tile), tile)
        v = jnp.dot(nf[r, :], inw[...], preferred_element_type=F32) * in_s[...]
        proj[r, :] = v.astype(BF16).astype(F32)
        return 0

    lax.fori_loop(0, 4, project, 0)

    v = proj[...]
    row = lax.broadcasted_iota(jnp.int32, v.shape, 0)

    def back(a, k):
        return jnp.where(row >= k, pltpu.roll(a, k, 0), 0.0)

    s2 = v + back(v, 1)
    s4 = s2 + back(s2, 2)
    s8 = s4 + back(s4, 4)
    s16 = s8 + back(s8, 8)
    total = jnp.where(x == 0, s2, jnp.where(x == 1, s4, jnp.where(x == 2, s8, s16)))
    count = jnp.minimum(row + 1, lax.shift_left(jnp.int32(2), x)).astype(F32)
    spread = (total / count - v).astype(BF16)
    mixed = jnp.dot(spread, pool_m[0], preferred_element_type=F32) * pool_s[...]
    pool[me] = mixed.astype(BF16)
    g_pool.start()

    go(2)
    g_pool.arrive(G.R0, G.L1)
    for j in range(1, tn):
        own_rows_copy(j, lax.rem(me + tn - j, tn), mate).wait_recv()
    for p in range(tn):
        for k in range(per):
            outw[p * chan : (p + 1) * chan, k * ocols : (k + 1) * ocols] = outg[p, k]
    g_pool.arrive(G.R1, G.L0)
    go(2)
    g_pool.arrive(G.F0, G.F1)
    g_pool.finish()

    def mix(i, _):
        r = pl.ds(pl.multiple_of(i * tile, tile), tile)
        rows = jnp.concatenate([pool[p, r, :] for p in range(tn)], axis=1)
        v = jnp.dot(rows, outw[...], preferred_element_type=F32)
        res[me, r, :] = (tok[me, r, :].astype(F32) + v).astype(BF16)
        return 0

    lax.fori_loop(0, 4, mix, 0)
    g_res.start()
    go(3)
    g_res.arrive(G.R0, G.L1)
    go(2)
    g_res.arrive(G.R1, G.L0)
    go(3)
    g_res.arrive(G.F0, G.F1)
    g_res.finish()
    go(1)
    norm(res, ffn_gain, 0, length // 2)
    go(2)
    norm(res, ffn_gain, length // 2, length)
    go(1)

    taps = lin.shape[0] - length

    def tile_product(at, n):
        def body(i, _):
            r = pl.ds(pl.multiple_of(i * tile, tile), tile)
            v = jnp.dot(nf[r, :], gu[:, pl.ds(at, n)], preferred_element_type=F32)
            v = (v * par[0:1, pl.ds(at, n)]).astype(BF16).astype(F32)
            lin[pl.ds(pl.multiple_of(taps + i * tile, 8), tile), 0:n] = v
            return 0

        lax.fori_loop(0, 4, body, 0)

    chunk = 64

    def convolved(i, at, off):
        w = lin[pl.ds(pl.multiple_of(i * chunk, 8), chunk + taps), off : off + LANES]
        t = par[:, pl.ds(at + off, LANES)]
        return (
            t[3:4] * w[taps:] + t[2:3] * pltpu.roll(w, 1, 0)[taps:] + t[1:2] * pltpu.roll(w, 2, 0)[taps:]
        )

    def silu(g):
        return g / (1.0 + jnp.exp(-g))

    def hcopy(j, which):
        ref = hid.at[which, j]
        return pltpu.make_async_remote_copy(
            ref, ref, hsend.at[j], hrecv.at[j], device_id={"tp": mate}, device_id_type=MESH
        )

    def column(j):
        at = pl.multiple_of(j * 2 * LANES, 2 * LANES)
        tile_product(at, 2 * LANES)

        def body(i, _):
            r = pl.ds(pl.multiple_of(i * chunk, chunk), chunk)
            h = silu(convolved(i, at, 0)) * convolved(i, at, LANES)
            hid[core, j, r, :] = h.astype(BF16)
            return 0

        lax.fori_loop(0, length // chunk, body, 0)
        hcopy(j, core).start()

    def two_columns(k, _):
        column(2 * k)
        tick(C1, k + 1)
        column(2 * k + 1)
        tick(C2, k + 1)
        return 0

    lax.fori_loop(0, full // 2, two_columns, 0)
    for j in range(full // 2 * 2, full):
        column(j)
    ahead = full // 2 + 1
    tick(C1, ahead)
    last = 2 * full * LANES
    tile_product(last, LANES)
    lane = lax.broadcasted_iota(jnp.int32, (chunk, LANES), 1)

    def narrow(i, _):
        r = pl.ds(pl.multiple_of(i * chunk, chunk), chunk)
        y = convolved(i, last, 0)
        h = jnp.where(lane < tail, silu(y) * pltpu.roll(y, LANES - tail, 1), 0.0)
        hid[core, full, r, :] = h.astype(BF16)
        return 0

    lax.fori_loop(0, length // chunk, narrow, 0)
    hcopy(full, core).start()
    tick(C2, ahead)

    def toward(m, p, src_chip):
        return pltpu.make_async_remote_copy(
            sbuf.at[m, p], rsb.at[src_chip, p], rsend.at[m, p], rrecv.at[src_chip, p],
            device_id={"tp": m * CORES + core}, device_id_type=MESH,
        )

    def block(slot):
        owner = lax.div(slot, per)
        m, p = lax.div(owner, CORES), lax.rem(slot, per)

        @pl.when(lax.rem(owner, CORES) == core)
        def _():
            def body(i, _):
                r = pl.ds(pl.multiple_of(i * tile, tile), tile)
                rows = jnp.concatenate([hid[k, j, r, :] for k in range(CORES) for j in range(full + 1)], axis=1)
                cols = jnp.concatenate([dn[k, slot] for k in range(CORES)], axis=0)
                sbuf[m, p, r, :] = jnp.dot(rows, cols, preferred_element_type=F32).astype(BF16)
                return 0

            lax.fori_loop(0, 4, body, 0)

            @pl.when(m != x)
            def _():
                toward(m, p, x).start()

    def pass_over(s):
        for d in range(2):
            hand(d, s, core, zslot(d, s)).start()

    def both(s):
        for d in range(2):
            slot = zslot(d, s)
            hand(d, s, other, slot).wait_recv()
            block(slot)

    lax.fori_loop(1, ahead + 1, lambda s, _: (pass_over(s), 0)[1], 0)
    for j in range(full + 1):
        hcopy(j, other).wait_recv()
    hand(0, 0, other, z).wait_recv()
    block(z)
    lax.fori_loop(1, ahead, lambda s, _: (both(s), 0)[1], 0)

    def onward(s, _):
        tick(C1, s)
        tick(C2, s)
        pass_over(s)
        both(s - 1)
        return 0

    lax.fori_loop(ahead + 1, hops - 1, onward, 0)
    onward(hops - 1, 0)
    both(hops - 1)
    tick(C1, hops)
    tick(C2, hops)
    end = zslot(0, hops)
    hand(0, hops, core, end).start()
    hand(0, hops, other, end).wait_recv()
    block(end)

    for j in range(1, chips):
        src = lax.rem(x + j, chips)
        for p in range(per):
            toward(x, p, src).wait_recv()

    def total_rows(i, _):
        r = pl.ds(pl.multiple_of(i * tile, tile), tile)
        for p in range(per):
            cols = slice(p * ocols, (p + 1) * ocols)
            v = res[me, r, cols].astype(F32) + sbuf[x, p, r, :].astype(F32)
            for j in range(1, chips):
                v = v + rsb[lax.rem(x + j, chips), p, r, :].astype(F32)
            out_ref[r, cols] = v.astype(BF16)
        return 0

    lax.fori_loop(0, 4, total_rows, 0)

    for g in gathers:
        g.drain()
    for j in range(1, tn):
        own_rows_copy(j, me, lax.rem(me + j, tn)).wait_send()
    for j in range(full + 1):
        hcopy(j, core).wait_send()
    hand(0, 0, core, z).wait_send()
    for s in range(1, hops):
        for d in range(2):
            hand(d, s, core, zslot(d, s)).wait_send()
    hand(0, hops, core, end).wait_send()
    for j in range(1, chips):
        for p in range(per):
            toward(lax.rem(x + j, chips), p, x).wait_send()


def layer(zn, tn, tokens, mix_gain, in_m, in_s, pool_m, pool_s, out_m, out_s, ffn_gain,
          gate_m, gate_s, up_m, up_s, gate_t, up_t, down_m, down_s):
    _, length, width = tokens.shape
    depth, chan = in_m.shape
    ff = gate_m.shape[1]
    ocols = out_m.shape[1]
    per = width // ocols
    assert ff % LANES == LANES // 2 and per == 2 and chan == LANES
    tiles = ff // LANES + 1
    chips = tn // CORES
    hops = zn // 2
    dma = pltpu.SemaphoreType.DMA
    vmem = pl.BlockSpec(memory_space=pltpu.VMEM)
    out = pl.pallas_call(
        functools.partial(kernel, zn, tn),
        out_shape=jax.ShapeDtypeStruct((length, width), BF16),
        in_specs=[pl.BlockSpec(memory_space=pl.ANY)] + [vmem] * 16,
        out_specs=vmem,
        scratch_shapes=[
            pltpu.VMEM((tn, length, width), BF16),
            pltpu.VMEM((tn, length, width), BF16),
            pltpu.VMEM((length, tn * width), BF16),
            pltpu.VMEM((zn, 2 * depth, chan), BF16),
            pltpu.VMEM((zn * depth, chan), BF16),
            pltpu.VMEM((tn, per, chan, ocols), BF16),
            pltpu.VMEM((tn * chan, width), BF16),
            pltpu.VMEM((length, chan), F32),
            pltpu.VMEM((tn, length, chan), BF16),
            pltpu.VMEM((zn * depth, 2 * ff), BF16),
            pltpu.VMEM((8, 2 * ff), F32),
            pltpu.VMEM((length + 8, 2 * LANES), F32),
            pltpu.VMEM((CORES, tiles, length, LANES), BF16),
            pltpu.VMEM((CORES, zn, tiles * LANES, ocols), BF16),
            pltpu.VMEM((chips, per, length, ocols), BF16),
            pltpu.VMEM((chips, per, length, ocols), BF16),
            dma,
            dma((6, 2)), dma((6, 2, hops)),
            dma((3, FeatureGather.TAGS)), dma((3, FeatureGather.TAGS)),
            dma((tn,)), dma((tn,)),
            dma((tiles,)), dma((tiles,)),
            dma((2, hops + 1)), dma((2, hops + 1)),
            dma((chips, per)), dma((chips, per)),
        ],
        compiler_params=pltpu.CompilerParams(
            collective_id=0, has_side_effects=True, vmem_limit_bytes=66_000_000
        ),
    )(
        tokens.reshape(length, width), mix_gain.reshape(1, -1), in_m, in_s, pool_m, pool_s, out_m, out_s,
        ffn_gain.reshape(1, -1), gate_m, gate_s, up_m, up_s, gate_t, up_t, down_m, down_s,
    )
    return out.reshape(tokens.shape)


def solution(mesh):
    return jax.shard_map(
        functools.partial(layer, mesh.shape["fs"], mesh.shape["tp"]),
        mesh=mesh,
        in_specs=(
            P(("grp", "fs"), None, "tp"),
            P(),
            P("fs", "tp"),
            P(None, "tp"),
            P("tp", None, None),
            P(None, "tp"),
            P("tp", "fs"),
            P(None, "fs"),
            P(),
            P("fs", "tp"),
            P(None, "tp"),
            P("fs", "tp"),
            P(None, "tp"),
            P(None, "tp"),
            P(None, "tp"),
            P("tp", "fs"),
            P(None, "fs"),
        ),
        out_specs=P(("grp", "fs"), None, "tp"),
        check_vma=False,
    )
```

```python
import functools

import jax
import jax.numpy as jnp
from jax import lax
from jax.experimental import pallas as pl
from jax.experimental.pallas import tpu as pltpu
from jax.sharding import PartitionSpec as P

MESH = pl.DeviceIdType.MESH
EPS = 1e-06
BF16 = jnp.bfloat16
F32 = jnp.float32
LANES = 128
CORES = 2


class FeatureGather:
    TAGS = 13
    R0, R1, L1, L0, F0, F1, OWN, PL0, PL1, PR0, PR1, PO0, PO1 = range(13)

    def __init__(self, buf, send, recv, chips, x, core):
        self.buf, self.send, self.recv = buf, send, recv
        self.half = buf.shape[1] // 2
        at = lambda chip, c: lax.rem(chip, chips) * CORES + c
        other = 1 - core
        self.me, self.mate = at(x, core), at(x, other)
        self.right, self.left, self.far = at(x + 1, core), at(x + chips - 1, core), at(x + 2, core)
        mright, mleft, mfar = at(x + 1, other), at(x + chips - 1, other), at(x + 2, other)
        self.out = {
            self.R0: (self.me, 0, self.right), self.R1: (self.me, 1, self.right),
            self.L1: (self.me, 1, self.left), self.L0: (self.me, 0, self.left),
            self.F0: (self.left, 0, self.right), self.F1: (self.right, 1, self.left),
            self.OWN: (self.me, None, self.mate),
            self.PL0: (self.left, 0, self.mate), self.PL1: (self.left, 1, self.mate),
            self.PR0: (self.right, 0, self.mate), self.PR1: (self.right, 1, self.mate),
            self.PO0: (self.far, 0, self.mate), self.PO1: (self.far, 1, self.mate),
        }
        self.inn = {
            self.R0: (self.left, 0), self.R1: (self.left, 1),
            self.L1: (self.right, 1), self.L0: (self.right, 0),
            self.F0: (self.far, 0), self.F1: (self.far, 1),
            self.OWN: (self.mate, None),
            self.PL0: (mleft, 0), self.PL1: (mleft, 1),
            self.PR0: (mright, 0), self.PR1: (mright, 1),
            self.PO0: (mfar, 0), self.PO1: (mfar, 1),
        }
        self.then = {
            self.R0: (self.F0, self.PL0), self.L1: (self.F1, self.PR1),
            self.R1: (self.PL1,), self.L0: (self.PR0,),
            self.F0: (self.PO0,), self.F1: (self.PO1,),
        }

    def ref(self, block, part):
        if part is None:
            return self.buf.at[block]
        return self.buf.at[block, pl.ds(part * self.half, self.half)]

    def copy(self, tag, block, part, to):
        ref = self.ref(block, part)
        return pltpu.make_async_remote_copy(
            ref, ref, self.send.at[tag], self.recv.at[tag], device_id={"tp": to}, device_id_type=MESH
        )

    def start(self):
        for tag in (self.R0, self.L1, self.R1, self.L0, self.OWN):
            self.copy(tag, *self.out[tag]).start()

    def arrive(self, *tags):
        for tag in tags:
            self.copy(tag, *self.inn[tag], self.mate).wait_recv()
            for later in self.then.get(tag, ()):
                self.copy(later, *self.out[later]).start()

    def finish(self):
        self.arrive(self.OWN, self.PL0, self.PR1, self.PL1, self.PR0, self.PO0, self.PO1)

    def drain(self):
        for tag in range(self.TAGS):
            self.copy(tag, *self.out[tag]).wait_send()


def kernel(
    zn, tn,
    tok_in, mix_gain, in_m, in_s, pool_m, pool_s, out_m, out_s, ffn_gain,
    gate_m, gate_s, up_m, up_s, gate_t, up_t, down_m, down_s,
    out_ref,
    tok, res, nf, io, inw, outg, outw, proj, pool, gu, par, lin, hid, dn, sums, far, near,
    load_sem, zsend, zrecv, gsend, grecv, osend, orecv, hsend, hrecv, dsend, drecv,
    ysend, yrecv, fsend, frecv, rsend, rrecv,
):
    z, me, group = lax.axis_index("fs"), lax.axis_index("tp"), lax.axis_index("grp")
    side = lax.rem(group, 2)
    twin = group + 1 - 2 * side
    x, core = lax.div(me, CORES), lax.rem(me, CORES)
    other = 1 - core
    mate = x * CORES + other
    chips = tn // CORES
    zright, zleft = lax.rem(z + 1, zn), lax.rem(z + zn - 1, zn)
    hops = zn // 2

    length, width = tok_in.shape
    depth, chan = in_m.shape
    ff = gate_m.shape[0]
    ocols = out_m.shape[1]
    full = ff // LANES
    tail = ff - full * LANES
    per = width // ocols

    load = pltpu.make_async_copy(tok_in, tok.at[me], load_sem)
    load.start()

    io[z, 0:depth, :] = in_m[...].astype(BF16)
    io[z, depth:, :] = (out_m[...] * out_s[...]).astype(BF16)

    def packed(g_ref, u_ref):
        for j in range(full):
            cols = slice(j * LANES, (j + 1) * LANES)
            yield 2 * j * LANES, jnp.concatenate([g_ref[:, cols], u_ref[:, cols]], axis=1)
        yield 2 * full * LANES, jnp.concatenate([g_ref[:, full * LANES :], u_ref[:, full * LANES :]], axis=1)

    own_rows = pl.ds(pl.multiple_of(z * depth, depth), depth)
    for j in range(full):
        for k, ref in enumerate((gate_m, up_m)):
            at = (2 * j + k) * LANES
            gu[own_rows, at : at + LANES] = ref[j * LANES : (j + 1) * LANES, :].T.astype(BF16)
    rest = jnp.concatenate([gate_m[full * LANES :, :], up_m[full * LANES :, :]], axis=0)
    gu[own_rows, 2 * full * LANES :] = rest.T.astype(BF16)
    for at, v in packed(gate_s, up_s):
        par[0:1, at : at + v.shape[1]] = v
    for at, v in packed(gate_t, up_t):
        par[1:4, at : at + v.shape[1]] = v
    dn[core, z, 0:ff, :] = (down_m[...] * down_s[...]).astype(BF16)
    dpad = dn.shape[2]

    def clear(i, _):
        dn[0, i, ff:dpad, :] = jnp.zeros((dpad - ff, ocols), BF16)
        dn[1, i, ff:dpad, :] = jnp.zeros((dpad - ff, ocols), BF16)
        return 0

    lax.fori_loop(0, zn, clear, 0)
    lin[0:8, :] = jnp.zeros((8, lin.shape[1]), F32)
    load.wait()

    barrier = pltpu.get_barrier_semaphore()
    for to in (zleft, zright):
        pl.semaphore_signal(barrier, inc=1, device_id={"fs": to}, device_id_type=MESH)
    for j in range(1, tn):
        pl.semaphore_signal(barrier, inc=1, device_id={"tp": lax.rem(me + j, tn)}, device_id_type=MESH)
    pl.semaphore_signal(barrier, inc=1, device_id={"grp": twin}, device_id_type=MESH)
    pl.semaphore_wait(barrier, tn + 2)

    def io_part(slot, part):
        n = 2 * depth
        if part is None:
            return io.at[slot]
        return io.at[slot, pl.ds(part * (n // 2), n // 2)]

    half = depth // 2
    cut = half // 2

    def gu_rows(b, slot, whose, part):
        a, m = (b * cut, cut) if part is None else (b * cut + part * (cut // 2), cut // 2)
        return gu.at[pl.ds(pl.multiple_of(slot * depth + whose * half + a, 16), m)]

    def gu_part(b):
        return lambda slot, part: gu_rows(b, slot, side, part)

    def dn_part(r0, n):
        def at(slot, part):
            a, m = (r0, n) if part is None else (r0 + part * (n // 2), n // 2)
            return dn.at[core, slot, pl.ds(a, m)]

        return at

    lanes = [io_part, gu_part(0), gu_part(1), dn_part(0, ff // 2), dn_part(ff // 2, ff // 2)]
    A, B1, B2, C1, C2 = range(5)

    def zslot(d, s):
        return lax.rem(z + zn + (s if d else -s), zn)

    def zcopy(i, d, s, part, slot):
        ref = lanes[i](slot, part)
        return pltpu.make_async_remote_copy(
            ref, ref, zsend.at[i, d], zrecv.at[i, d, s - 1],
            device_id={"fs": zleft if d else zright}, device_id_type=MESH,
        )

    def zput(i, d, s, part=None):
        return zcopy(i, d, s, part, zslot(d, s - 1))

    def zgot(i, d, s, part=None):
        zcopy(i, d, s, part, zslot(d, s)).wait_recv()

    def zopen(i):
        for d in range(2):
            zput(i, d, 1).start()

    def tick(i, s):
        for d in range(2):
            static = isinstance(s, int)
            part = d if static and s == hops else None
            zgot(i, d, s, part)
            zput(i, d, s, part).wait_send()
            if not static or s < hops - 1:
                zput(i, d, s + 1).start()
            elif s == hops - 1:
                zput(i, d, s + 1, d).start()
            if not static or s < hops:
                handed(i, d, s)
        if isinstance(s, int) and s == hops:
            handed(i, 0, s)

    def ycopy(b, d, s, whose):
        ref = gu_rows(b, zslot(d, s), whose, None)
        return pltpu.make_async_remote_copy(
            ref, ref, ysend.at[b, d, s], yrecv.at[b, d, s], device_id={"grp": twin}, device_id_type=MESH
        )

    def hand(c, d, s, which):
        ref = dn.at[which, zslot(d, s), pl.ds(c * (ff // 2), ff // 2)]
        return pltpu.make_async_remote_copy(
            ref, ref, dsend.at[c, d, s], drecv.at[c, d, s], device_id={"tp": mate}, device_id_type=MESH
        )

    def ocopy(slot, src):
        owner = lax.div(slot, per)
        return pltpu.make_async_remote_copy(
            io.at[slot, pl.ds(depth, depth)], outg.at[src, lax.rem(slot, per)],
            osend.at[slot], orecv.at[src, lax.rem(slot, per)],
            device_id={"tp": owner}, device_id_type=MESH,
        )

    def handed(i, d, s):
        if i == A:
            slot = zslot(d, s)

            @pl.when(lax.div(slot, per) != me)
            def _():
                ocopy(slot, me).start()
        elif i in (B1, B2):
            ycopy(i - B1, d, s, side).start()
        else:
            hand(i - C1, d, s, core).start()


    def each_arrival(fn):
        fn(0, 0)

        def body(s, _):
            fn(0, s)
            fn(1, s)
            return 0

        lax.fori_loop(1, hops, body, 0)
        fn(0, hops)

    def steps():
        for s in range(1, hops + 1):
            tick(A, s)
            if s == hops - 1:
                zopen(B2)
            tick(B1, s)
            if s == hops - 1:
                zopen(C1)
            yield
        for s in range(1, hops + 1):
            tick(B2, s)
            tick(C1, s)
            if s == hops - 2:
                zopen(C2)
            if s > hops - 2:
                tick(C2, s + 2 - hops)
            yield

    ring = steps()

    def go(n):
        for _ in range(n):
            next(ring)

    gathers = [
        FeatureGather(buf, gsend.at[k], grecv.at[k], chips, x, core) for k, buf in enumerate((tok, pool, res))
    ]
    g_tok, g_pool, g_res = gathers
    G = FeatureGather

    zopen(A)
    zopen(B1)
    g_tok.start()
    for i in (A, B1, B2, C1, C2):
        handed(i, 0, 0)

    def norm(buf, gain_ref, lo, hi):
        rows = 32

        def body(i, _):
            r = pl.ds(pl.multiple_of(i * rows, rows), rows)
            total = jnp.zeros((rows, width), F32)
            for p in range(tn):
                v = buf[p, r, :].astype(F32)
                total = total + v * v
            mean = jnp.sum(total, axis=1, keepdims=True) * (1.0 / (tn * width))
            scale = lax.rsqrt(mean + EPS)
            for p in range(tn):
                cols = slice(p * width, (p + 1) * width)
                nf[r, cols] = (buf[p, r, :].astype(F32) * scale * gain_ref[:, cols]).astype(BF16)
            return 0

        lax.fori_loop(lo // rows, hi // rows, body, 0)

    go(2)
    g_tok.arrive(G.R0, G.L1)
    go(1)
    g_tok.arrive(G.R1, G.L0)
    go(2)
    g_tok.arrive(G.F0, G.F1)
    g_tok.finish()
    part = length // 4
    norm(tok, mix_gain, 0, part)
    go(1)
    norm(tok, mix_gain, part, 2 * part)
    norm(tok, mix_gain, 2 * part, 3 * part)
    go(1)
    norm(tok, mix_gain, 3 * part, length)
    go(1)

    for k in range(zn):
        inw[k * depth : (k + 1) * depth, :] = io[k, 0:depth, :]
    tile = length // 4

    def project(i, _):
        r = pl.ds(pl.multiple_of(i * tile, tile), tile)
        v = jnp.dot(nf[r, :], inw[...], preferred_element_type=F32) * in_s[...]
        proj[r, :] = v.astype(BF16).astype(F32)
        return 0

    lax.fori_loop(0, 4, project, 0)

    v = proj[...]
    row = lax.broadcasted_iota(jnp.int32, v.shape, 0)

    def back(a, k):
        return jnp.where(row >= k, pltpu.roll(a, k, 0), 0.0)

    s2 = v + back(v, 1)
    s4 = s2 + back(s2, 2)
    s8 = s4 + back(s4, 4)
    s16 = s8 + back(s8, 8)
    total = jnp.where(x == 0, s2, jnp.where(x == 1, s4, jnp.where(x == 2, s8, s16)))
    count = jnp.minimum(row + 1, lax.shift_left(jnp.int32(2), x)).astype(F32)
    spread = (total / count - v).astype(BF16)
    mixed = jnp.dot(spread, pool_m[0], preferred_element_type=F32) * pool_s[...]
    pool[me] = mixed.astype(BF16)
    g_pool.start()

    go(1)
    g_pool.arrive(G.R0, G.L1)

    def others(fn):
        for j in range(1, tn):
            for k in range(per):
                fn(lax.rem(me + j, tn), k)

    others(lambda p, k: ocopy(me * per + k, p).wait_recv())
    for k in range(per):
        outg[me, k] = io[me * per + k, depth:, :]
    for p in range(tn):
        for k in range(per):
            outw[p * chan : (p + 1) * chan, k * ocols : (k + 1) * ocols] = outg[p, k]
    go(1)
    g_pool.arrive(G.R1, G.L0)
    g_pool.arrive(G.F0, G.F1)
    go(1)
    g_pool.finish()

    def mix(i, _):
        r = pl.ds(pl.multiple_of(i * tile, tile), tile)
        rows = jnp.concatenate([pool[p, r, :] for p in range(tn)], axis=1)
        v = jnp.dot(rows, outw[...], preferred_element_type=F32)
        res[me, r, :] = (tok[me, r, :].astype(F32) + v).astype(BF16)
        return 0

    lax.fori_loop(0, 4, mix, 0)
    g_res.start()
    go(2)
    g_res.arrive(G.R0, G.L1)
    go(1)
    g_res.arrive(G.R1, G.L0)
    go(1)
    g_res.arrive(G.F0, G.F1)
    g_res.finish()
    norm(res, ffn_gain, 0, length // 2)
    go(1)
    norm(res, ffn_gain, length // 2, length)
    for b in range(2):
        each_arrival(lambda d, s, b=b: ycopy(b, d, s, 1 - side).wait_recv())

    taps = lin.shape[0] - length

    def tile_product(at, n):
        def body(i, _):
            r = pl.ds(pl.multiple_of(i * tile, tile), tile)
            v = jnp.dot(nf[r, :], gu[:, pl.ds(at, n)], preferred_element_type=F32)
            v = (v * par[0:1, pl.ds(at, n)]).astype(BF16).astype(F32)
            lin[pl.ds(pl.multiple_of(taps + i * tile, 8), tile), 0:n] = v
            return 0

        lax.fori_loop(0, 4, body, 0)

    chunk = 64

    def convolved(i, at, off):
        w = lin[pl.ds(pl.multiple_of(i * chunk, 8), chunk + taps), off : off + LANES]
        t = par[:, pl.ds(at + off, LANES)]
        return (
            t[3:4] * w[taps:] + t[2:3] * pltpu.roll(w, 1, 0)[taps:] + t[1:2] * pltpu.roll(w, 2, 0)[taps:]
        )

    def silu(g):
        return g / (1.0 + jnp.exp(-g))

    def hcopy(j, which):
        ref = hid.at[which, j]
        return pltpu.make_async_remote_copy(
            ref, ref, hsend.at[j], hrecv.at[j], device_id={"tp": mate}, device_id_type=MESH
        )

    def column(j):
        at = pl.multiple_of(j * 2 * LANES, 2 * LANES)
        tile_product(at, 2 * LANES)

        def body(i, _):
            r = pl.ds(pl.multiple_of(i * chunk, chunk), chunk)
            h = silu(convolved(i, at, 0)) * convolved(i, at, LANES)
            hid[core, j, r, :] = h.astype(BF16)
            return 0

        lax.fori_loop(0, length // chunk, body, 0)
        hcopy(j, core).start()

    early = 3

    def some_columns(j, _):
        column(j)
        tick(C2, j + early)
        return 0

    lax.fori_loop(0, full - 1, some_columns, 0)
    column(full - 1)
    tick(C2, full - 1 + early)
    last = 2 * full * LANES
    tile_product(last, LANES)
    lane = lax.broadcasted_iota(jnp.int32, (chunk, LANES), 1)

    def narrow(i, _):
        r = pl.ds(pl.multiple_of(i * chunk, chunk), chunk)
        y = convolved(i, last, 0)
        h = jnp.where(lane < tail, silu(y) * pltpu.roll(y, LANES - tail, 1), 0.0)
        hid[core, full, r, :] = h.astype(BF16)
        return 0

    lax.fori_loop(0, length // chunk, narrow, 0)
    hcopy(full, core).start()
    tick(C2, hops)

    for j in range(full + 1):
        hcopy(j, other).wait_recv()
    for c in range(2):
        each_arrival(lambda d, s, c=c: hand(c, d, s, other).wait_recv())

    at_chip = lambda m: lax.rem(m, chips) * CORES + core
    FAR, RIGHT, LEFT, OWN = range(4)
    owner_of = (x + 2, x + 1, x + chips - 1, x)
    side_rows = length // 2

    def down(which, h, extra=None):
        m = lax.rem(owner_of[which], chips)
        slot = (m * CORES + core) * per

        def body(i, _):
            r = pl.ds(pl.multiple_of(h * side_rows + i * tile, tile), tile)
            rows = jnp.concatenate([hid[k, j, r, :] for k in range(CORES) for j in range(full + 1)], axis=1)
            cols = jnp.concatenate(
                [jnp.concatenate([dn[k, slot + p] for p in range(per)], axis=1) for k in range(CORES)], axis=0
            )
            v = jnp.dot(rows, cols, preferred_element_type=F32)
            if extra is not None:
                v = v + far[extra, pl.ds(pl.multiple_of(i * tile, tile), tile), :].astype(F32)
            sums[which, r, :] = v.astype(BF16)
            return 0

        lax.fori_loop(0, side_rows // tile, body, 0)

    def half_rows(h):
        return pl.ds(h * side_rows, side_rows)

    def far_copy(h):
        return pltpu.make_async_remote_copy(
            sums.at[FAR, half_rows(h)], far.at[h], fsend.at[h], frecv.at[h],
            device_id={"tp": at_chip(x + chips - 1 if h else x + 1)}, device_id_type=MESH,
        )

    def near_copy(which, h):
        k = which - RIGHT
        return pltpu.make_async_remote_copy(
            sums.at[which, half_rows(h)], near.at[k, half_rows(h)], rsend.at[k, h], rrecv.at[k, h],
            device_id={"tp": at_chip(owner_of[which])}, device_id_type=MESH,
        )

    down(FAR, 0)
    far_copy(0).start()
    down(FAR, 1)
    far_copy(1).start()
    down(RIGHT, 1)
    near_copy(RIGHT, 1).start()
    down(LEFT, 0)
    near_copy(LEFT, 0).start()
    down(OWN, 0)
    far_copy(0).wait_recv()
    down(RIGHT, 0, 0)
    near_copy(RIGHT, 0).start()
    far_copy(1).wait_recv()
    down(LEFT, 1, 1)
    near_copy(LEFT, 1).start()
    down(OWN, 1)

    def total_rows(h):
        def body(i, _):
            r = pl.ds(pl.multiple_of(h * side_rows + i * tile, tile), tile)
            v = res[me, r, :].astype(F32) + sums[OWN, r, :].astype(F32)
            for k in range(2):
                v = v + near[k, r, :].astype(F32)
            out_ref[r, :] = v.astype(BF16)
            return 0

        lax.fori_loop(0, side_rows // tile, body, 0)

    for which, h in ((RIGHT, 1), (LEFT, 0), (RIGHT, 0), (LEFT, 1)):
        near_copy(which, h).wait_recv()
    for h in range(2):
        total_rows(h)

    for g in gathers:
        g.drain()
    for j in range(full + 1):
        hcopy(j, core).wait_send()

    def outs_left(slot, _):
        @pl.when(lax.div(slot, per) != me)
        def _():
            ocopy(slot, me).wait_send()

        return 0

    lax.fori_loop(0, zn, outs_left, 0)
    for b in range(2):
        each_arrival(lambda d, s, b=b: ycopy(b, d, s, side).wait_send())
        each_arrival(lambda d, s, b=b: hand(b, d, s, core).wait_send())
    for h in range(2):
        far_copy(h).wait_send()
        near_copy(RIGHT, h).wait_send()
        near_copy(LEFT, h).wait_send()


def layer(gn, zn, tn, tokens, mix_gain, in_m, in_s, pool_m, pool_s, out_m, out_s, ffn_gain,
          gate_m, gate_s, up_m, up_s, gate_t, up_t, down_m, down_s):
    _, length, width = tokens.shape
    depth, chan = in_m.shape
    ff = gate_m.shape[1]
    ocols = out_m.shape[1]
    per = width // ocols
    assert ff % LANES == LANES // 2 and per == 2 and chan == LANES and tn == 4 * CORES and gn % 2 == 0
    tiles = ff // LANES + 1
    hops = zn // 2
    dma = pltpu.SemaphoreType.DMA
    vmem = pl.BlockSpec(memory_space=pltpu.VMEM)
    out = pl.pallas_call(
        functools.partial(kernel, zn, tn),
        out_shape=jax.ShapeDtypeStruct((length, width), BF16),
        in_specs=[pl.BlockSpec(memory_space=pl.ANY)] + [vmem] * 16,
        out_specs=vmem,
        scratch_shapes=[
            pltpu.VMEM((tn, length, width), BF16),
            pltpu.VMEM((tn, length, width), BF16),
            pltpu.VMEM((length, tn * width), BF16),
            pltpu.VMEM((zn, 2 * depth, chan), BF16),
            pltpu.VMEM((zn * depth, chan), BF16),
            pltpu.VMEM((tn, per, chan, ocols), BF16),
            pltpu.VMEM((tn * chan, width), BF16),
            pltpu.VMEM((length, chan), F32),
            pltpu.VMEM((tn, length, chan), BF16),
            pltpu.VMEM((zn * depth, 2 * ff), BF16),
            pltpu.VMEM((8, 2 * ff), F32),
            pltpu.VMEM((length + 8, 2 * LANES), F32),
            pltpu.VMEM((CORES, tiles, length, LANES), BF16),
            pltpu.VMEM((CORES, zn, tiles * LANES, ocols), BF16),
            pltpu.VMEM((4, length, width), BF16),
            pltpu.VMEM((2, length // 2, width), BF16),
            pltpu.VMEM((2, length, width), BF16),
            dma,
            dma((5, 2)), dma((5, 2, hops)),
            dma((3, FeatureGather.TAGS)), dma((3, FeatureGather.TAGS)),
            dma((zn,)), dma((tn, per)),
            dma((tiles,)), dma((tiles,)),
            dma((2, 2, hops + 1)), dma((2, 2, hops + 1)),
            dma((2, 2, hops + 1)), dma((2, 2, hops + 1)),
            dma((2,)), dma((2,)),
            dma((2, 2)), dma((2, 2)),
        ],
        compiler_params=pltpu.CompilerParams(
            collective_id=0, has_side_effects=True, vmem_limit_bytes=66_000_000
        ),
    )(
        tokens.reshape(length, width), mix_gain.reshape(1, -1), in_m, in_s, pool_m, pool_s, out_m, out_s,
        ffn_gain.reshape(1, -1), gate_m.T, gate_s, up_m.T, up_s, gate_t, up_t, down_m, down_s,
    )
    return out.reshape(tokens.shape)


def solution(mesh):
    return jax.shard_map(
        functools.partial(layer, mesh.shape["grp"], mesh.shape["fs"], mesh.shape["tp"]),
        mesh=mesh,
        in_specs=(
            P(("grp", "fs"), None, "tp"),
            P(),
            P("fs", "tp"),
            P(None, "tp"),
            P("tp", None, None),
            P(None, "tp"),
            P("tp", "fs"),
            P(None, "fs"),
            P(),
            P("fs", "tp"),
            P(None, "tp"),
            P("fs", "tp"),
            P(None, "tp"),
            P(None, "tp"),
            P(None, "tp"),
            P("tp", "fs"),
            P(None, "fs"),
        ),
        out_specs=P(("grp", "fs"), None, "tp"),
        check_vma=False,
    )
```

```python
import functools

import jax
import jax.numpy as jnp
from jax import lax
from jax.experimental import pallas as pl
from jax.experimental.pallas import tpu as pltpu
from jax.sharding import PartitionSpec as P

MESH = pl.DeviceIdType.MESH
EPS = 1e-06
BF16 = jnp.bfloat16
F32 = jnp.float32
LANES = 128
CORES = 2
ROUTE = {
    1: (0, 1), 15: (0, -1), 2: (0, 2), 14: (0, -2), 4: (0, 4), 12: (0, -4), 8: (0, 8),
    5: (4, 1), 3: (4, -1), 6: (4, 2), 13: (12, 1), 11: (12, -1), 10: (12, -2), 9: (8, 1), 7: (8, -1),
}


class FeatureGather:
    TAGS = 13
    R0, R1, L1, L0, F0, F1, OWN, PL0, PL1, PR0, PR1, PO0, PO1 = range(13)

    def __init__(self, buf, send, recv, chips, x, core, base, count):
        self.buf, self.send, self.recv = buf, send, recv
        self.base, self.half = base, count // 2
        at = lambda chip, c: lax.rem(chip, chips) * CORES + c
        other = 1 - core
        self.me, self.mate = at(x, core), at(x, other)
        self.right, self.left, self.far = at(x + 1, core), at(x + chips - 1, core), at(x + 2, core)
        mright, mleft, mfar = at(x + 1, other), at(x + chips - 1, other), at(x + 2, other)
        self.out = {
            self.R0: (self.me, 0, self.right), self.R1: (self.me, 1, self.right),
            self.L1: (self.me, 1, self.left), self.L0: (self.me, 0, self.left),
            self.F0: (self.left, 0, self.right), self.F1: (self.right, 1, self.left),
            self.OWN: (self.me, None, self.mate),
            self.PL0: (self.left, 0, self.mate), self.PL1: (self.left, 1, self.mate),
            self.PR0: (self.right, 0, self.mate), self.PR1: (self.right, 1, self.mate),
            self.PO0: (self.far, 0, self.mate), self.PO1: (self.far, 1, self.mate),
        }
        self.inn = {
            self.R0: (self.left, 0), self.R1: (self.left, 1),
            self.L1: (self.right, 1), self.L0: (self.right, 0),
            self.F0: (self.far, 0), self.F1: (self.far, 1),
            self.OWN: (self.mate, None),
            self.PL0: (mleft, 0), self.PL1: (mleft, 1),
            self.PR0: (mright, 0), self.PR1: (mright, 1),
            self.PO0: (mfar, 0), self.PO1: (mfar, 1),
        }
        self.then = {
            self.R0: (self.F0, self.PL0), self.L1: (self.F1, self.PR1),
            self.R1: (self.PL1,), self.L0: (self.PR0,),
            self.F0: (self.PO0,), self.F1: (self.PO1,),
        }

    def ref(self, block, part):
        if part is None:
            return self.buf.at[block, pl.ds(self.base, 2 * self.half)]
        return self.buf.at[block, pl.ds(self.base + part * self.half, self.half)]

    def copy(self, tag, block, part, to):
        ref = self.ref(block, part)
        return pltpu.make_async_remote_copy(
            ref, ref, self.send.at[tag], self.recv.at[tag], device_id={"tp": to}, device_id_type=MESH
        )

    def start(self):
        for tag in (self.R0, self.L1, self.R1, self.L0, self.OWN):
            self.copy(tag, *self.out[tag]).start()

    def arrive(self, *tags):
        for tag in tags:
            self.copy(tag, *self.inn[tag], self.mate).wait_recv()
            for later in self.then.get(tag, ()):
                self.copy(later, *self.out[later]).start()

    def finish(self):
        self.arrive(self.OWN, self.PL0, self.PR1, self.PL1, self.PR0, self.PO0, self.PO1)

    def drain(self):
        for tag in range(self.TAGS):
            self.copy(tag, *self.out[tag]).wait_send()


def kernel(
    zn, tn,
    tok_in, mix_gain, in_m, in_s, pool_m, pool_s, out_m, out_s, ffn_gain,
    gate_m, gate_s, up_m, up_s, gate_t, up_t, down_m, down_s,
    out_ref,
    tok, res, nf, io, inw, outg, outw, proj, pool, gu, par, lin, edge, hid, dn, sums, far, near,
    load_sem, zsend, zrecv, gsend, grecv, osend, orecv, hsend, hrecv, dsend, drecv,
    ysend, yrecv, asend, arecv, xsend, xrecv, fsend, frecv, rsend, rrecv,
):
    z, me, group = lax.axis_index("fs"), lax.axis_index("tp"), lax.axis_index("grp")
    side = lax.rem(group, 2)
    twin = group + 1 - 2 * side
    x, core = lax.div(me, CORES), lax.rem(me, CORES)
    other = 1 - core
    mate = x * CORES + other
    chips = tn // CORES
    zright, zleft = lax.rem(z + 1, zn), lax.rem(z + zn - 1, zn)
    hops = zn // 2

    length, width = tok_in.shape
    depth, chan = in_m.shape
    ff = gate_m.shape[0]
    ocols = out_m.shape[1]
    full = ff // LANES
    tail = ff - full * LANES
    per = width // ocols

    load = pltpu.make_async_copy(tok_in, tok.at[me], load_sem)
    load.start()

    half = depth // 2
    scaled_out = (out_m[...] * out_s[...]).astype(BF16)
    for k in range(2):
        io[z, k, 0:half, :] = in_m[k * half : (k + 1) * half, :].astype(BF16)
        io[z, k, half:, :] = scaled_out[k * half : (k + 1) * half]

    def packed(g_ref, u_ref):
        for j in range(full):
            cols = slice(j * LANES, (j + 1) * LANES)
            yield 2 * j * LANES, jnp.concatenate([g_ref[:, cols], u_ref[:, cols]], axis=1)
        yield 2 * full * LANES, jnp.concatenate([g_ref[:, full * LANES :], u_ref[:, full * LANES :]], axis=1)

    own_rows = pl.ds(pl.multiple_of(z * depth, depth), depth)
    for j in range(full):
        for k, ref in enumerate((gate_m, up_m)):
            at = (2 * j + k) * LANES
            gu[own_rows, at : at + LANES] = ref[j * LANES : (j + 1) * LANES, :].T.astype(BF16)
    rest = jnp.concatenate([gate_m[full * LANES :, :], up_m[full * LANES :, :]], axis=0)
    gu[own_rows, 2 * full * LANES :] = rest.T.astype(BF16)
    for at, v in packed(gate_s, up_s):
        par[0:1, at : at + v.shape[1]] = v
    for at, v in packed(gate_t, up_t):
        par[1:4, at : at + v.shape[1]] = v
    dn[core, z, 0:ff, :] = (down_m[...] * down_s[...]).astype(BF16)
    dpad = dn.shape[2]

    def clear(i, _):
        dn[0, i, ff:dpad, :] = jnp.zeros((dpad - ff, ocols), BF16)
        dn[1, i, ff:dpad, :] = jnp.zeros((dpad - ff, ocols), BF16)
        return 0

    lax.fori_loop(0, zn, clear, 0)
    edge[...] = jnp.zeros(edge.shape, F32)
    load.wait()

    barrier = pltpu.get_barrier_semaphore()
    reach = sorted({o for _, o in ROUTE.values()})
    for o in reach:
        pl.semaphore_signal(barrier, inc=1, device_id={"fs": lax.rem(z + o + zn, zn)}, device_id_type=MESH)
    for j in range(1, tn):
        pl.semaphore_signal(barrier, inc=1, device_id={"tp": lax.rem(me + j, tn)}, device_id_type=MESH)
    pl.semaphore_signal(barrier, inc=1, device_id={"grp": twin}, device_id_type=MESH)
    pl.semaphore_wait(barrier, tn + len(reach))

    shared = 3 * depth // 8
    common = depth - 2 * shared

    def gu_ref(slot, a, m):
        return gu.at[pl.ds(pl.multiple_of(slot * depth + a, 16), m)]

    def gu_shared(slot, part, whose):
        n = 2 * shared // 3
        a, m = ((0, shared), (0, n), (n, shared - n))[0 if part is None else part + 1]
        return gu_ref(slot, whose * shared + a, m)

    def gu_common(slot, part):
        a, m = (0, common) if part is None else (part * (common // 2), common // 2)
        return gu_ref(slot, 2 * shared + a, m)

    def dn_part(r0, n):
        def at(slot, part):
            a, m = (r0, n) if part is None else (r0 + part * (n // 2), n // 2)
            return dn.at[core, slot, pl.ds(a, m)]

        return at

    lanes = [
        lambda slot, part: gu_shared(slot, part, side), gu_common,
        dn_part(0, ff // 2), dn_part(ff // 2, ff // 2),
    ]
    B1, B2, C1, C2 = range(4)

    def zslot(d, s):
        return lax.rem(z + zn + (s if d else -s), zn)

    def zcopy(i, d, s, part, slot):
        ref = lanes[i](slot, part)
        return pltpu.make_async_remote_copy(
            ref, ref, zsend.at[i, d], zrecv.at[i, d, s - 1],
            device_id={"fs": zleft if d else zright}, device_id_type=MESH,
        )

    def zput(i, d, s, part=None):
        return zcopy(i, d, s, part, zslot(d, s - 1))

    def zgot(i, d, s, part=None):
        zcopy(i, d, s, part, zslot(d, s)).wait_recv()

    def zopen(i):
        for d in range(2):
            zput(i, d, 1).start()

    def tick(i, s):
        for d in range(2):
            static = isinstance(s, int)
            part = d if static and s == hops else None
            zgot(i, d, s, part)
            zput(i, d, s, part).wait_send()
            if not static or s < hops - 1:
                zput(i, d, s + 1).start()
            elif s == hops - 1:
                zput(i, d, s + 1, d).start()
            if not static or s < hops:
                handed(i, d, s)
        if isinstance(s, int) and s == hops:
            handed(i, 0, s)

    def ycopy(d, s, whose):
        ref = gu_shared(zslot(d, s), None, whose)
        return pltpu.make_async_remote_copy(
            ref, ref, ysend.at[d, s], yrecv.at[d, s], device_id={"grp": twin}, device_id_type=MESH
        )

    def hand(c, d, s, which):
        ref = dn.at[which, zslot(d, s), pl.ds(c * (ff // 2), ff // 2)]
        return pltpu.make_async_remote_copy(
            ref, ref, dsend.at[c, d, s], drecv.at[c, d, s], device_id={"tp": mate}, device_id_type=MESH
        )

    def ocopy(slot, src):
        owner = lax.div(slot, per)
        return pltpu.make_async_remote_copy(
            io.at[slot, pl.ds(0, 2), pl.ds(half, half)], outg.at[src, lax.rem(slot, per)],
            osend.at[slot], orecv.at[src, lax.rem(slot, per)],
            device_id={"tp": owner}, device_id_type=MESH,
        )

    def handed(i, d, s):
        if i == B1:
            if not (isinstance(s, int) and s == 1):
                ycopy(d, s, side).start()
        elif i in (C1, C2):
            hand(i - C1, d, s, core).start()

    def acopy(off, sending):
        behind, o = ROUTE[off]
        slot = lax.rem(z - (behind if sending else off) + zn, zn)
        ref = io.at[slot, side]
        return pltpu.make_async_remote_copy(
            ref, ref, asend.at[off], arecv.at[off],
            device_id={"fs": lax.rem(z + o + zn, zn)}, device_id_type=MESH,
        )

    def across(off, whose):
        ref = io.at[lax.rem(z - off + zn, zn), whose]
        return pltpu.make_async_remote_copy(
            ref, ref, xsend.at[off], xrecv.at[off], device_id={"grp": twin}, device_id_type=MESH
        )

    def aput(behind):
        for off, (b, _) in ROUTE.items():
            if b == behind:
                acopy(off, True).start()

    def agot(*offs):
        for off in offs:
            acopy(off, False).wait_recv()
            if off in (4, 12, 8):
                aput(off)
            across(off, side).start()

    def a_all():
        for off in ROUTE:
            across(off, 1 - side).wait_recv()

        def body(slot, _):
            @pl.when(lax.div(slot, per) != me)
            def _():
                ocopy(slot, me).start()

            return 0

        lax.fori_loop(0, zn, body, 0)

    def each_arrival(fn, own=True):
        if own:
            fn(0, 0)

        def body(s, _):
            fn(0, s)
            fn(1, s)
            return 0

        lax.fori_loop(1, hops, body, 0)
        fn(0, hops)

    def steps():
        for first, second in ((B1, B2), (C1, C2)):
            for s in range(1, hops + 1):
                tick(first, s)
                if first == B1 and s == hops - 1:
                    zopen(C1)
                tick(second, s)
                if first == B1 and s == hops - 1:
                    zopen(C2)
                yield

    ring = steps()

    def go(n):
        for _ in range(n):
            next(ring)

    gathers = [
        FeatureGather(buf, gsend.at[k], grecv.at[k], chips, x, core, base, count)
        for k, (buf, base, count) in enumerate(
            ((tok, 0, length), (pool, 0, length), (res, 0, length // 2), (res, length // 2, length // 2))
        )
    ]
    g_tok, g_pool, g_first, g_second = gathers
    G = FeatureGather

    aput(0)
    zopen(B1)
    zopen(B2)
    g_tok.start()
    for i in (C1, C2):
        handed(i, 0, 0)

    def norm(buf, gain_ref, lo, hi):
        rows = 32

        def body(i, _):
            r = pl.ds(pl.multiple_of(i * rows, rows), rows)
            total = jnp.zeros((rows, width), F32)
            for p in range(tn):
                v = buf[p, r, :].astype(F32)
                total = total + v * v
            mean = jnp.sum(total, axis=1, keepdims=True) * (1.0 / (tn * width))
            scale = lax.rsqrt(mean + EPS)
            for p in range(tn):
                cols = slice(p * width, (p + 1) * width)
                nf[r, cols] = (buf[p, r, :].astype(F32) * scale * gain_ref[:, cols]).astype(BF16)
            return 0

        lax.fori_loop(lo // rows, hi // rows, body, 0)

    agot(1, 15, 2, 14)
    agot(4, 12)
    g_tok.arrive(G.R0, G.L1)
    agot(8)
    go(1)
    agot(5, 3, 6, 13, 11, 10)
    agot(9, 7)
    for d in range(2):
        ycopy(d, 1, side).start()
    g_tok.arrive(G.R1, G.L0)
    go(1)
    a_all()
    g_tok.arrive(G.F0, G.F1)
    g_tok.finish()
    part = length // 4
    norm(tok, mix_gain, 0, part)
    norm(tok, mix_gain, part, 2 * part)
    norm(tok, mix_gain, 2 * part, 3 * part)
    norm(tok, mix_gain, 3 * part, length)
    go(1)

    for k in range(zn):
        for h in range(2):
            inw[k * depth + h * half : k * depth + (h + 1) * half, :] = io[k, h, 0:half, :]
    tile = length // 4

    def project(i, _):
        r = pl.ds(pl.multiple_of(i * tile, tile), tile)
        v = jnp.dot(nf[r, :], inw[...], preferred_element_type=F32) * in_s[...]
        proj[r, :] = v.astype(BF16).astype(F32)
        return 0

    lax.fori_loop(0, 4, project, 0)

    v = proj[...]
    row = lax.broadcasted_iota(jnp.int32, v.shape, 0)

    def back(a, k):
        return jnp.where(row >= k, pltpu.roll(a, k, 0), 0.0)

    s2 = v + back(v, 1)
    s4 = s2 + back(s2, 2)
    s8 = s4 + back(s4, 4)
    s16 = s8 + back(s8, 8)
    total = jnp.where(x == 0, s2, jnp.where(x == 1, s4, jnp.where(x == 2, s8, s16)))
    count = jnp.minimum(row + 1, lax.shift_left(jnp.int32(2), x)).astype(F32)
    spread = (total / count - v).astype(BF16)
    mixed = jnp.dot(spread, pool_m[0], preferred_element_type=F32) * pool_s[...]
    pool[me] = mixed.astype(BF16)
    g_pool.start()

    go(1)
    g_pool.arrive(G.R0, G.L1)

    def others(fn):
        for j in range(1, tn):
            for k in range(per):
                fn(lax.rem(me + j, tn), k)

    others(lambda p, k: ocopy(me * per + k, p).wait_recv())
    for k in range(per):
        outg[me, k] = io[me * per + k, :, half:, :]
    for p in range(tn):
        for k in range(per):
            for h in range(2):
                rows = slice(p * chan + h * half, p * chan + (h + 1) * half)
                outw[rows, k * ocols : (k + 1) * ocols] = outg[p, k, h]
    go(1)
    g_pool.arrive(G.R1, G.L0)
    g_pool.arrive(G.F0, G.F1)
    go(1)
    g_pool.finish()

    def mix(i, _):
        r = pl.ds(pl.multiple_of(i * tile, tile), tile)
        rows = jnp.concatenate([pool[p, r, :] for p in range(tn)], axis=1)
        v = jnp.dot(rows, outw[...], preferred_element_type=F32)
        res[me, r, :] = (tok[me, r, :].astype(F32) + v).astype(BF16)
        return 0

    lax.fori_loop(0, 2, mix, 0)
    g_first.start()
    lax.fori_loop(2, 4, mix, 0)
    go(1)
    g_first.arrive(G.R0, G.L1)
    g_second.start()
    go(1)
    g_first.arrive(G.R1, G.L0)
    g_first.arrive(G.F0, G.F1)
    go(1)
    g_first.finish()
    norm(res, ffn_gain, 0, length // 2)

    def both_down(s):
        tick(C1, s)
        tick(C2, s)

    g_second.arrive(G.R0, G.L1)
    both_down(2)
    each_arrival(lambda d, s: ycopy(d, s, 1 - side).wait_recv(), own=False)

    side_rows = length // 2
    taps = lin.shape[0] - side_rows

    def tile_product(h, j, at, n):
        lin[0:taps, 0:n] = edge[j, :, 0:n]

        def body(i, _):
            r = pl.ds(pl.multiple_of(h * side_rows + i * tile, tile), tile)
            v = jnp.dot(nf[r, :], gu[:, pl.ds(at, n)], preferred_element_type=F32)
            v = (v * par[0:1, pl.ds(at, n)]).astype(BF16).astype(F32)
            lin[pl.ds(pl.multiple_of(taps + i * tile, 8), tile), 0:n] = v
            return 0

        lax.fori_loop(0, side_rows // tile, body, 0)
        edge[j, :, 0:n] = lin[side_rows:, 0:n]

    chunk = 64

    def convolved(i, at, off):
        w = lin[pl.ds(pl.multiple_of(i * chunk, 8), chunk + taps), off : off + LANES]
        t = par[:, pl.ds(at + off, LANES)]
        return (
            t[3:4] * w[taps:] + t[2:3] * pltpu.roll(w, 1, 0)[taps:] + t[1:2] * pltpu.roll(w, 2, 0)[taps:]
        )

    def silu(g):
        return g / (1.0 + jnp.exp(-g))

    def hcopy(h, j, which):
        ref = hid.at[which, j, pl.ds(h * side_rows, side_rows)]
        return pltpu.make_async_remote_copy(
            ref, ref, hsend.at[h, j], hrecv.at[h, j], device_id={"tp": mate}, device_id_type=MESH
        )

    def store_rows(h, i):
        return pl.ds(pl.multiple_of(h * side_rows + i * chunk, chunk), chunk)

    def column(h, j):
        at = pl.multiple_of(j * 2 * LANES, 2 * LANES)
        tile_product(h, j, at, 2 * LANES)

        def body(i, _):
            v = silu(convolved(i, at, 0)) * convolved(i, at, LANES)
            hid[core, j, store_rows(h, i), :] = v.astype(BF16)
            return 0

        lax.fori_loop(0, side_rows // chunk, body, 0)
        hcopy(h, j, core).start()

    last = 2 * full * LANES
    lane = lax.broadcasted_iota(jnp.int32, (chunk, LANES), 1)

    def narrow_column(h):
        tile_product(h, full, last, LANES)

        def body(i, _):
            y = convolved(i, last, 0)
            v = jnp.where(lane < tail, silu(y) * pltpu.roll(y, LANES - tail, 1), 0.0)
            hid[core, full, store_rows(h, i), :] = v.astype(BF16)
            return 0

        lax.fori_loop(0, side_rows // chunk, body, 0)
        hcopy(h, full, core).start()

    def feed(h, after):
        def body(j, _):
            column(h, j)
            after(j)
            return 0

        lax.fori_loop(0, full, body, 0)
        narrow_column(h)

    def after_first(j):
        @pl.when(j == 0)
        def _():
            g_second.arrive(G.R1, G.L0)

        @pl.when(j == 1)
        def _():
            both_down(3)

        @pl.when(j == 2)
        def _():
            g_second.arrive(G.F0, G.F1)

        @pl.when(j == 4)
        def _():
            both_down(4)

    def after_second(j):
        @pl.when(j == 2)
        def _():
            both_down(6)

    feed(0, after_first)
    g_second.finish()
    norm(res, ffn_gain, side_rows, length)
    both_down(5)
    feed(1, after_second)
    both_down(hops - 1)
    both_down(hops)

    for j in range(full + 1):
        for h in range(2):
            hcopy(h, j, other).wait_recv()
    for c in range(2):
        each_arrival(lambda d, s, c=c: hand(c, d, s, other).wait_recv())

    at_chip = lambda m: lax.rem(m, chips) * CORES + core
    FAR, RIGHT, LEFT, OWN = range(4)
    owner_of = (x + 2, x + 1, x + chips - 1, x)

    def down(which, h, extra=None):
        m = lax.rem(owner_of[which], chips)
        slot = (m * CORES + core) * per

        def body(i, _):
            r = pl.ds(pl.multiple_of(h * side_rows + i * tile, tile), tile)
            rows = jnp.concatenate([hid[k, j, r, :] for k in range(CORES) for j in range(full + 1)], axis=1)
            cols = jnp.concatenate(
                [jnp.concatenate([dn[k, slot + p] for p in range(per)], axis=1) for k in range(CORES)], axis=0
            )
            v = jnp.dot(rows, cols, preferred_element_type=F32)
            if extra is not None:
                v = v + far[extra, pl.ds(pl.multiple_of(i * tile, tile), tile), :].astype(F32)
            sums[which, r, :] = v.astype(BF16)
            return 0

        lax.fori_loop(0, side_rows // tile, body, 0)

    def half_rows(h):
        return pl.ds(h * side_rows, side_rows)

    def far_copy(h):
        return pltpu.make_async_remote_copy(
            sums.at[FAR, half_rows(h)], far.at[h], fsend.at[h], frecv.at[h],
            device_id={"tp": at_chip(x + chips - 1 if h else x + 1)}, device_id_type=MESH,
        )

    def near_copy(which, h):
        k = which - RIGHT
        return pltpu.make_async_remote_copy(
            sums.at[which, half_rows(h)], near.at[k, half_rows(h)], rsend.at[k, h], rrecv.at[k, h],
            device_id={"tp": at_chip(owner_of[which])}, device_id_type=MESH,
        )

    down(FAR, 0)
    far_copy(0).start()
    down(FAR, 1)
    far_copy(1).start()
    down(RIGHT, 1)
    near_copy(RIGHT, 1).start()
    down(LEFT, 0)
    near_copy(LEFT, 0).start()
    down(OWN, 0)
    far_copy(0).wait_recv()
    down(RIGHT, 0, 0)
    near_copy(RIGHT, 0).start()
    far_copy(1).wait_recv()
    down(LEFT, 1, 1)
    near_copy(LEFT, 1).start()
    down(OWN, 1)

    def total_rows(h):
        def body(i, _):
            r = pl.ds(pl.multiple_of(h * side_rows + i * tile, tile), tile)
            v = res[me, r, :].astype(F32) + sums[OWN, r, :].astype(F32)
            for k in range(2):
                v = v + near[k, r, :].astype(F32)
            out_ref[r, :] = v.astype(BF16)
            return 0

        lax.fori_loop(0, side_rows // tile, body, 0)

    for which, h in ((RIGHT, 1), (LEFT, 0), (RIGHT, 0), (LEFT, 1)):
        near_copy(which, h).wait_recv()
    for h in range(2):
        total_rows(h)

    for g in gathers:
        g.drain()
    for j in range(full + 1):
        for h in range(2):
            hcopy(h, j, core).wait_send()

    def outs_left(slot, _):
        @pl.when(lax.div(slot, per) != me)
        def _():
            ocopy(slot, me).wait_send()

        return 0

    lax.fori_loop(0, zn, outs_left, 0)
    each_arrival(lambda d, s: ycopy(d, s, side).wait_send(), own=False)
    for off in ROUTE:
        across(off, side).wait_send()
        acopy(off, True).wait_send()
    for b in range(2):
        each_arrival(lambda d, s, b=b: hand(b, d, s, core).wait_send())
    for h in range(2):
        far_copy(h).wait_send()
        near_copy(RIGHT, h).wait_send()
        near_copy(LEFT, h).wait_send()


def layer(gn, zn, tn, tokens, mix_gain, in_m, in_s, pool_m, pool_s, out_m, out_s, ffn_gain,
          gate_m, gate_s, up_m, up_s, gate_t, up_t, down_m, down_s):
    _, length, width = tokens.shape
    depth, chan = in_m.shape
    ff = gate_m.shape[1]
    ocols = out_m.shape[1]
    per = width // ocols
    assert ff % LANES == LANES // 2 and per == 2 and chan == LANES and tn == 4 * CORES and gn % 2 == 0 and zn == 16
    tiles = ff // LANES + 1
    hops = zn // 2
    dma = pltpu.SemaphoreType.DMA
    vmem = pl.BlockSpec(memory_space=pltpu.VMEM)
    out = pl.pallas_call(
        functools.partial(kernel, zn, tn),
        out_shape=jax.ShapeDtypeStruct((length, width), BF16),
        in_specs=[pl.BlockSpec(memory_space=pl.ANY)] + [vmem] * 16,
        out_specs=vmem,
        scratch_shapes=[
            pltpu.VMEM((tn, length, width), BF16),
            pltpu.VMEM((tn, length, width), BF16),
            pltpu.VMEM((length, tn * width), BF16),
            pltpu.VMEM((zn, 2, depth, chan), BF16),
            pltpu.VMEM((zn * depth, chan), BF16),
            pltpu.VMEM((tn, per, 2, chan // 2, ocols), BF16),
            pltpu.VMEM((tn * chan, width), BF16),
            pltpu.VMEM((length, chan), F32),
            pltpu.VMEM((tn, length, chan), BF16),
            pltpu.VMEM((zn * depth, 2 * ff), BF16),
            pltpu.VMEM((8, 2 * ff), F32),
            pltpu.VMEM((length // 2 + 8, 2 * LANES), F32),
            pltpu.VMEM((tiles, 8, 2 * LANES), F32),
            pltpu.VMEM((CORES, tiles, length, LANES), BF16),
            pltpu.VMEM((CORES, zn, tiles * LANES, ocols), BF16),
            pltpu.VMEM((4, length, width), BF16),
            pltpu.VMEM((2, length // 2, width), BF16),
            pltpu.VMEM((2, length, width), BF16),
            dma,
            dma((4, 2)), dma((4, 2, hops)),
            dma((4, FeatureGather.TAGS)), dma((4, FeatureGather.TAGS)),
            dma((zn,)), dma((tn, per)),
            dma((2, tiles)), dma((2, tiles)),
            dma((2, 2, hops + 1)), dma((2, 2, hops + 1)),
            dma((2, hops + 1)), dma((2, hops + 1)),
            dma((zn,)), dma((zn,)), dma((zn,)), dma((zn,)),
            dma((2,)), dma((2,)),
            dma((2, 2)), dma((2, 2)),
        ],
        compiler_params=pltpu.CompilerParams(
            collective_id=0, has_side_effects=True, vmem_limit_bytes=66_000_000
        ),
    )(
        tokens.reshape(length, width), mix_gain.reshape(1, -1), in_m, in_s, pool_m, pool_s, out_m, out_s,
        ffn_gain.reshape(1, -1), gate_m.T, gate_s, up_m.T, up_s, gate_t, up_t, down_m, down_s,
    )
    return out.reshape(tokens.shape)


def solution(mesh):
    return jax.shard_map(
        functools.partial(layer, mesh.shape["grp"], mesh.shape["fs"], mesh.shape["tp"]),
        mesh=mesh,
        in_specs=(
            P(("grp", "fs"), None, "tp"),
            P(),
            P("fs", "tp"),
            P(None, "tp"),
            P("tp", None, None),
            P(None, "tp"),
            P("tp", "fs"),
            P(None, "fs"),
            P(),
            P("fs", "tp"),
            P(None, "tp"),
            P("fs", "tp"),
            P(None, "tp"),
            P(None, "tp"),
            P(None, "tp"),
            P("tp", "fs"),
            P(None, "fs"),
        ),
        out_specs=P(("grp", "fs"), None, "tp"),
        check_vma=False,
    )
```

```python
import functools

import jax
import jax.numpy as jnp
from jax import lax
from jax.experimental import pallas as pl
from jax.experimental.pallas import tpu as pltpu
from jax.sharding import PartitionSpec as P

MESH = pl.DeviceIdType.MESH
EPS = 1e-06
BF16 = jnp.bfloat16
F32 = jnp.float32
LANES = 128
CORES = 2
ROUTE = {
    1: (0, 1), 15: (0, -1), 2: (0, 2), 14: (0, -2), 4: (0, 4), 12: (0, -4),
    5: (4, 1), 3: (4, -1), 6: (4, 2), 13: (12, 1), 11: (12, -1), 10: (12, -2), 9: (8, 1), 7: (8, -1),
}
QUARTER, OPPOSITE = 4, 8
BEHIND = (*ROUTE, OPPOSITE)


class FeatureGather:
    TAGS = 13
    R0, R1, L1, L0, F0, F1, OWN, PL0, PL1, PR0, PR1, PO0, PO1 = range(13)

    def __init__(self, buf, send, recv, chips, x, core, base, count):
        self.buf, self.send, self.recv = buf, send, recv
        self.base, self.half = base, count // 2
        at = lambda chip, c: lax.rem(chip, chips) * CORES + c
        other = 1 - core
        self.me, self.mate = at(x, core), at(x, other)
        self.right, self.left, self.far = at(x + 1, core), at(x + chips - 1, core), at(x + 2, core)
        mright, mleft, mfar = at(x + 1, other), at(x + chips - 1, other), at(x + 2, other)
        self.out = {
            self.R0: (self.me, 0, self.right), self.R1: (self.me, 1, self.right),
            self.L1: (self.me, 1, self.left), self.L0: (self.me, 0, self.left),
            self.F0: (self.left, 0, self.right), self.F1: (self.right, 1, self.left),
            self.OWN: (self.me, None, self.mate),
            self.PL0: (self.left, 0, self.mate), self.PL1: (self.left, 1, self.mate),
            self.PR0: (self.right, 0, self.mate), self.PR1: (self.right, 1, self.mate),
            self.PO0: (self.far, 0, self.mate), self.PO1: (self.far, 1, self.mate),
        }
        self.inn = {
            self.R0: (self.left, 0), self.R1: (self.left, 1),
            self.L1: (self.right, 1), self.L0: (self.right, 0),
            self.F0: (self.far, 0), self.F1: (self.far, 1),
            self.OWN: (self.mate, None),
            self.PL0: (mleft, 0), self.PL1: (mleft, 1),
            self.PR0: (mright, 0), self.PR1: (mright, 1),
            self.PO0: (mfar, 0), self.PO1: (mfar, 1),
        }
        self.then = {
            self.R0: (self.F0, self.PL0), self.L1: (self.F1, self.PR1),
            self.R1: (self.PL1,), self.L0: (self.PR0,),
            self.F0: (self.PO0,), self.F1: (self.PO1,),
        }

    def ref(self, block, part):
        if part is None:
            return self.buf.at[block, pl.ds(self.base, 2 * self.half)]
        return self.buf.at[block, pl.ds(self.base + part * self.half, self.half)]

    def copy(self, tag, block, part, to):
        ref = self.ref(block, part)
        return pltpu.make_async_remote_copy(
            ref, ref, self.send.at[tag], self.recv.at[tag], device_id={"tp": to}, device_id_type=MESH
        )

    def start(self):
        for tag in (self.R0, self.L1, self.R1, self.L0, self.OWN):
            self.copy(tag, *self.out[tag]).start()

    def arrive(self, *tags):
        for tag in tags:
            self.copy(tag, *self.inn[tag], self.mate).wait_recv()
            for later in self.then.get(tag, ()):
                self.copy(later, *self.out[later]).start()

    def finish(self):
        self.arrive(self.OWN, self.PL0, self.PR1, self.PL1, self.PR0, self.PO0, self.PO1)

    def drain(self):
        for tag in range(self.TAGS):
            self.copy(tag, *self.out[tag]).wait_send()


def kernel(
    zn, tn,
    tok_in, mix_gain, in_m, in_s, pool_m, pool_s, out_m, out_s, ffn_gain,
    gate_m, gate_s, up_m, up_s, gate_t, up_t, down_m, down_s,
    out_ref,
    tok, res, nf, io, inw, outg, outw, proj, pool, gu, par, lin, edge, hid, dn, sums, far, near,
    load_sem, zsend, zrecv, gsend, grecv, osend, orecv, hsend, hrecv, dsend, drecv,
    ysend, yrecv, asend, arecv, esend, erecv, xsend, xrecv, fsend, frecv, rsend, rrecv,
):
    z, me, group = lax.axis_index("fs"), lax.axis_index("tp"), lax.axis_index("grp")
    side = lax.rem(group, 2)
    twin = group + 1 - 2 * side
    x, core = lax.div(me, CORES), lax.rem(me, CORES)
    other = 1 - core
    mate = x * CORES + other
    chips = tn // CORES
    zright, zleft = lax.rem(z + 1, zn), lax.rem(z + zn - 1, zn)
    hops = zn // 2

    length, width = tok_in.shape
    depth, chan = in_m.shape
    ff = gate_m.shape[0]
    ocols = out_m.shape[1]
    full = ff // LANES
    tail = ff - full * LANES
    per = width // ocols

    barrier = pltpu.get_barrier_semaphore()
    reach = sorted({o for _, o in ROUTE.values()})
    for o in reach:
        pl.semaphore_signal(barrier, inc=1, device_id={"fs": lax.rem(z + o + zn, zn)}, device_id_type=MESH)
    for j in range(1, tn):
        pl.semaphore_signal(barrier, inc=1, device_id={"tp": lax.rem(me + j, tn)}, device_id_type=MESH)
    pl.semaphore_signal(barrier, inc=1, device_id={"grp": twin}, device_id_type=MESH)

    load = pltpu.make_async_copy(tok_in, tok.at[me], load_sem)
    load.start()

    half = depth // 2
    scaled_out = (out_m[...] * out_s[...]).astype(BF16)
    for k in range(2):
        io[z, k, 0:half, :] = in_m[k * half : (k + 1) * half, :].astype(BF16)
        io[z, k, half:, :] = scaled_out[k * half : (k + 1) * half]

    def packed(g_ref, u_ref):
        for j in range(full):
            cols = slice(j * LANES, (j + 1) * LANES)
            yield 2 * j * LANES, jnp.concatenate([g_ref[:, cols], u_ref[:, cols]], axis=1)
        yield 2 * full * LANES, jnp.concatenate([g_ref[:, full * LANES :], u_ref[:, full * LANES :]], axis=1)

    own_rows = pl.ds(pl.multiple_of(z * depth, depth), depth)
    for j in range(full):
        for k, ref in enumerate((gate_m, up_m)):
            at = (2 * j + k) * LANES
            gu[own_rows, at : at + LANES] = ref[j * LANES : (j + 1) * LANES, :].T.astype(BF16)
    rest = jnp.concatenate([gate_m[full * LANES :, :], up_m[full * LANES :, :]], axis=0)
    gu[own_rows, 2 * full * LANES :] = rest.T.astype(BF16)
    for at, v in packed(gate_s, up_s):
        par[0:1, at : at + v.shape[1]] = v
    for at, v in packed(gate_t, up_t):
        par[1:4, at : at + v.shape[1]] = v
    dn[core, z, 0:ff, :] = (down_m[...] * down_s[...]).astype(BF16)
    dpad = dn.shape[2]

    def clear(i, _):
        dn[0, i, ff:dpad, :] = jnp.zeros((dpad - ff, ocols), BF16)
        dn[1, i, ff:dpad, :] = jnp.zeros((dpad - ff, ocols), BF16)
        return 0

    lax.fori_loop(0, zn, clear, 0)
    edge[...] = jnp.zeros(edge.shape, F32)
    load.wait()

    pl.semaphore_wait(barrier, tn + len(reach))

    shared = 3 * depth // 8
    common = depth - 2 * shared

    def gu_ref(slot, a, m):
        return gu.at[pl.ds(pl.multiple_of(slot * depth + a, 16), m)]

    def gu_shared(slot, part, whose):
        n = 2 * shared // 3
        a, m = ((0, shared), (0, n), (n, shared - n))[0 if part is None else part + 1]
        return gu_ref(slot, whose * shared + a, m)

    def gu_common(slot, part):
        a, m = (0, common) if part is None else (part * (common // 2), common // 2)
        return gu_ref(slot, 2 * shared + a, m)

    def dn_part(r0, n):
        def at(slot, part):
            a, m = (r0, n) if part is None else (r0 + part * (n // 2), n // 2)
            return dn.at[core, slot, pl.ds(a, m)]

        return at

    lanes = [
        lambda slot, part: gu_shared(slot, part, side), gu_common,
        dn_part(0, ff // 2), dn_part(ff // 2, ff // 2),
    ]
    B1, B2, C1, C2 = range(4)

    def zslot(d, s):
        return lax.rem(z + zn + (s if d else -s), zn)

    def zcopy(i, d, s, part, slot):
        ref = lanes[i](slot, part)
        return pltpu.make_async_remote_copy(
            ref, ref, zsend.at[i, d], zrecv.at[i, d, s - 1],
            device_id={"fs": zleft if d else zright}, device_id_type=MESH,
        )

    def zput(i, d, s, part=None):
        return zcopy(i, d, s, part, zslot(d, s - 1))

    def zgot(i, d, s, part=None):
        zcopy(i, d, s, part, zslot(d, s)).wait_recv()

    def zopen(i):
        for d in range(2):
            zput(i, d, 1).start()

    def tick(i, s):
        for d in range(2):
            static = isinstance(s, int)
            part = d if static and s == hops else None
            zgot(i, d, s, part)
            zput(i, d, s, part).wait_send()
            if not static or s < hops - 1:
                zput(i, d, s + 1).start()
            elif s == hops - 1:
                zput(i, d, s + 1, d).start()
            if not static or s < hops:
                handed(i, d, s)
        if isinstance(s, int) and s == hops:
            handed(i, 0, s)

    def ycopy(d, s, whose):
        ref = gu_shared(zslot(d, s), None, whose)
        return pltpu.make_async_remote_copy(
            ref, ref, ysend.at[d, s], yrecv.at[d, s], device_id={"grp": twin}, device_id_type=MESH
        )

    def hand(c, d, s, which):
        ref = dn.at[which, zslot(d, s), pl.ds(c * (ff // 2), ff // 2)]
        return pltpu.make_async_remote_copy(
            ref, ref, dsend.at[c, d, s], drecv.at[c, d, s], device_id={"tp": mate}, device_id_type=MESH
        )

    def ocopy(slot, src):
        owner = lax.div(slot, per)
        return pltpu.make_async_remote_copy(
            io.at[slot, pl.ds(0, 2), pl.ds(half, half)], outg.at[src, lax.rem(slot, per)],
            osend.at[slot], orecv.at[src, lax.rem(slot, per)],
            device_id={"tp": owner}, device_id_type=MESH,
        )

    def handed(i, d, s):
        if i == B1:
            if not (isinstance(s, int) and s == 1):
                ycopy(d, s, side).start()
        elif i in (C1, C2):
            hand(i - C1, d, s, core).start()

    def acopy(off, sending):
        behind, o = ROUTE[off]
        slot = lax.rem(z - (behind if sending else off) + zn, zn)
        ref = io.at[slot, side]
        return pltpu.make_async_remote_copy(
            ref, ref, asend.at[off], arecv.at[off],
            device_id={"fs": lax.rem(z + o + zn, zn)}, device_id_type=MESH,
        )

    def across(off, whose):
        ref = io.at[lax.rem(z - off + zn, zn), whose]
        return pltpu.make_async_remote_copy(
            ref, ref, xsend.at[off], xrecv.at[off], device_id={"grp": twin}, device_id_type=MESH
        )

    def aput(behind):
        for off, (b, _) in sorted(ROUTE.items(), key=lambda r: r[0] not in (QUARTER, -QUARTER % zn)):
            if b == behind:
                acopy(off, True).start()

    def agot(*offs):
        for off in offs:
            acopy(off, False).wait_recv()
            if off in (QUARTER, -QUARTER % zn):
                opposite(int(off != QUARTER), True).start()
                aput(off)
            across(off, side).start()

    def opposite(k, sending):
        o = -QUARTER if k else QUARTER
        slot = lax.rem(z + (-o if sending else OPPOSITE) + zn, zn)
        ref = io.at[slot, side, pl.ds(k * half, half)]
        return pltpu.make_async_remote_copy(
            ref, ref, esend.at[k], erecv.at[k],
            device_id={"fs": lax.rem(z + o + zn, zn)}, device_id_type=MESH,
        )

    def opposite_got():
        for k in range(2):
            opposite(k, False).wait_recv()
        aput(OPPOSITE)
        across(OPPOSITE, side).start()

    def a_all():
        for off in BEHIND:
            across(off, 1 - side).wait_recv()

        def body(slot, _):
            @pl.when(lax.div(slot, per) != me)
            def _():
                ocopy(slot, me).start()

            return 0

        lax.fori_loop(0, zn, body, 0)

    def each_arrival(fn, own=True):
        if own:
            fn(0, 0)

        def body(s, _):
            fn(0, s)
            fn(1, s)
            return 0

        lax.fori_loop(1, hops, body, 0)
        fn(0, hops)

    def steps():
        for first, second in ((B1, B2), (C1, C2)):
            for s in range(1, hops + 1):
                tick(first, s)
                if first == B1 and s == hops - 1:
                    zopen(C1)
                tick(second, s)
                if first == B1 and s == hops - 1:
                    zopen(C2)
                yield

    ring = steps()

    def go(n):
        for _ in range(n):
            next(ring)

    gathers = [
        FeatureGather(buf, gsend.at[k], grecv.at[k], chips, x, core, base, count)
        for k, (buf, base, count) in enumerate(
            ((tok, 0, length), (pool, 0, length), (res, 0, length // 2), (res, length // 2, length // 2))
        )
    ]
    g_tok, g_pool, g_first, g_second = gathers
    G = FeatureGather

    aput(0)
    zopen(B1)
    zopen(B2)
    g_tok.start()
    for i in (C1, C2):
        handed(i, 0, 0)

    def norm(buf, gain_ref, lo, hi):
        rows = 32

        def body(i, _):
            r = pl.ds(pl.multiple_of(i * rows, rows), rows)
            total = jnp.zeros((rows, width), F32)
            for p in range(tn):
                v = buf[p, r, :].astype(F32)
                total = total + v * v
            mean = jnp.sum(total, axis=1, keepdims=True) * (1.0 / (tn * width))
            scale = lax.rsqrt(mean + EPS)
            for p in range(tn):
                cols = slice(p * width, (p + 1) * width)
                nf[r, cols] = (buf[p, r, :].astype(F32) * scale * gain_ref[:, cols]).astype(BF16)
            return 0

        lax.fori_loop(lo // rows, hi // rows, body, 0)

    agot(4, 12)
    agot(1, 15, 2, 14)
    g_tok.arrive(G.R0, G.L1)
    opposite_got()
    go(1)
    agot(5, 3, 6, 13, 11, 10)
    agot(9, 7)
    for d in range(2):
        ycopy(d, 1, side).start()
    g_tok.arrive(G.R1, G.L0)
    go(1)
    a_all()
    g_tok.arrive(G.F0, G.F1)
    g_tok.finish()
    part = length // 4
    norm(tok, mix_gain, 0, part)
    norm(tok, mix_gain, part, 2 * part)
    go(1)
    norm(tok, mix_gain, 2 * part, 3 * part)
    norm(tok, mix_gain, 3 * part, length)

    for k in range(zn):
        for h in range(2):
            inw[k * depth + h * half : k * depth + (h + 1) * half, :] = io[k, h, 0:half, :]
    tile = length // 4

    def project(i, _):
        r = pl.ds(pl.multiple_of(i * tile, tile), tile)
        v = jnp.dot(nf[r, :], inw[...], preferred_element_type=F32) * in_s[...]
        proj[r, :] = v.astype(BF16).astype(F32)
        return 0

    lax.fori_loop(0, 4, project, 0)

    v = proj[...]
    row = lax.broadcasted_iota(jnp.int32, v.shape, 0)

    def back(a, k):
        return jnp.where(row >= k, pltpu.roll(a, k, 0), 0.0)

    s2 = v + back(v, 1)
    s4 = s2 + back(s2, 2)
    s8 = s4 + back(s4, 4)
    s16 = s8 + back(s8, 8)
    total = jnp.where(x == 0, s2, jnp.where(x == 1, s4, jnp.where(x == 2, s8, s16)))
    count = jnp.minimum(row + 1, lax.shift_left(jnp.int32(2), x)).astype(F32)
    spread = (total / count - v).astype(BF16)
    mixed = jnp.dot(spread, pool_m[0], preferred_element_type=F32) * pool_s[...]
    pool[me] = mixed.astype(BF16)
    g_pool.start()

    go(1)
    g_pool.arrive(G.R0, G.L1)

    def others(fn):
        for j in range(1, tn):
            for k in range(per):
                fn(lax.rem(me + j, tn), k)

    others(lambda p, k: ocopy(me * per + k, p).wait_recv())
    for k in range(per):
        outg[me, k] = io[me * per + k, :, half:, :]
    for p in range(tn):
        for k in range(per):
            for h in range(2):
                rows = slice(p * chan + h * half, p * chan + (h + 1) * half)
                outw[rows, k * ocols : (k + 1) * ocols] = outg[p, k, h]
    go(1)
    g_pool.arrive(G.R1, G.L0)
    g_pool.arrive(G.F0, G.F1)
    g_pool.finish()

    def mix(i, _):
        r = pl.ds(pl.multiple_of(i * tile, tile), tile)
        rows = jnp.concatenate([pool[p, r, :] for p in range(tn)], axis=1)
        v = jnp.dot(rows, outw[...], preferred_element_type=F32)
        res[me, r, :] = (tok[me, r, :].astype(F32) + v).astype(BF16)
        return 0

    lax.fori_loop(0, 2, mix, 0)
    g_first.start()
    lax.fori_loop(2, 4, mix, 0)
    go(2)
    g_first.arrive(G.R0, G.L1)
    g_second.start()
    go(1)
    g_first.arrive(G.R1, G.L0)
    g_first.arrive(G.F0, G.F1)
    go(1)
    g_first.finish()
    norm(res, ffn_gain, 0, length // 2)

    def both_down(s):
        tick(C1, s)
        tick(C2, s)

    g_second.arrive(G.R0, G.L1)
    both_down(2)
    each_arrival(lambda d, s: ycopy(d, s, 1 - side).wait_recv(), own=False)

    side_rows = length // 2
    taps = lin.shape[0] - side_rows

    def tile_product(h, j, at, n):
        lin[0:taps, 0:n] = edge[j, :, 0:n]

        def body(i, _):
            r = pl.ds(pl.multiple_of(h * side_rows + i * tile, tile), tile)
            v = jnp.dot(nf[r, :], gu[:, pl.ds(at, n)], preferred_element_type=F32)
            v = (v * par[0:1, pl.ds(at, n)]).astype(BF16).astype(F32)
            lin[pl.ds(pl.multiple_of(taps + i * tile, 8), tile), 0:n] = v
            return 0

        lax.fori_loop(0, side_rows // tile, body, 0)
        edge[j, :, 0:n] = lin[side_rows:, 0:n]

    chunk = 64

    def convolved(i, at, off):
        w = lin[pl.ds(pl.multiple_of(i * chunk, 8), chunk + taps), off : off + LANES]
        t = par[:, pl.ds(at + off, LANES)]
        return (
            t[3:4] * w[taps:] + t[2:3] * pltpu.roll(w, 1, 0)[taps:] + t[1:2] * pltpu.roll(w, 2, 0)[taps:]
        )

    def silu(g):
        return g / (1.0 + jnp.exp(-g))

    def hcopy(h, j, which):
        ref = hid.at[which, j, pl.ds(h * side_rows, side_rows)]
        return pltpu.make_async_remote_copy(
            ref, ref, hsend.at[h, j], hrecv.at[h, j], device_id={"tp": mate}, device_id_type=MESH
        )

    def store_rows(h, i):
        return pl.ds(pl.multiple_of(h * side_rows + i * chunk, chunk), chunk)

    def column(h, j):
        at = pl.multiple_of(j * 2 * LANES, 2 * LANES)
        tile_product(h, j, at, 2 * LANES)

        def body(i, _):
            v = silu(convolved(i, at, 0)) * convolved(i, at, LANES)
            hid[core, j, store_rows(h, i), :] = v.astype(BF16)
            return 0

        lax.fori_loop(0, side_rows // chunk, body, 0)
        hcopy(h, j, core).start()

    last = 2 * full * LANES
    lane = lax.broadcasted_iota(jnp.int32, (chunk, LANES), 1)

    def narrow_column(h):
        tile_product(h, full, last, LANES)

        def body(i, _):
            y = convolved(i, last, 0)
            v = jnp.where(lane < tail, silu(y) * pltpu.roll(y, LANES - tail, 1), 0.0)
            hid[core, full, store_rows(h, i), :] = v.astype(BF16)
            return 0

        lax.fori_loop(0, side_rows // chunk, body, 0)
        hcopy(h, full, core).start()

    def feed(h, after):
        def body(j, _):
            column(h, j)
            after(j)
            return 0

        lax.fori_loop(0, full, body, 0)
        narrow_column(h)

    def after_first(j):
        @pl.when(j == 0)
        def _():
            g_second.arrive(G.R1, G.L0)

        @pl.when(j == 1)
        def _():
            both_down(3)

        @pl.when(j == 2)
        def _():
            g_second.arrive(G.F0, G.F1)

        @pl.when(j == 4)
        def _():
            both_down(4)

    def after_second(j):
        @pl.when(j == 1)
        def _():
            both_down(6)

        @pl.when(j == 4)
        def _():
            both_down(hops - 1)

    feed(0, after_first)
    g_second.finish()
    norm(res, ffn_gain, side_rows, length)
    both_down(5)
    feed(1, after_second)
    both_down(hops)

    for j in range(full + 1):
        for h in range(2):
            hcopy(h, j, other).wait_recv()
    for c in range(2):
        each_arrival(lambda d, s, c=c: hand(c, d, s, other).wait_recv())

    at_chip = lambda m: lax.rem(m, chips) * CORES + core
    FAR, RIGHT, LEFT, OWN = range(4)
    owner_of = (x + 2, x + 1, x + chips - 1, x)

    def down(which, h, extra=None):
        m = lax.rem(owner_of[which], chips)
        slot = (m * CORES + core) * per

        def body(i, _):
            r = pl.ds(pl.multiple_of(h * side_rows + i * tile, tile), tile)
            rows = jnp.concatenate([hid[k, j, r, :] for k in range(CORES) for j in range(full + 1)], axis=1)
            cols = jnp.concatenate(
                [jnp.concatenate([dn[k, slot + p] for p in range(per)], axis=1) for k in range(CORES)], axis=0
            )
            v = jnp.dot(rows, cols, preferred_element_type=F32)
            if extra is not None:
                v = v + far[extra, pl.ds(pl.multiple_of(i * tile, tile), tile), :].astype(F32)
            sums[which, r, :] = v.astype(BF16)
            return 0

        lax.fori_loop(0, side_rows // tile, body, 0)

    def half_rows(h):
        return pl.ds(h * side_rows, side_rows)

    def far_copy(h):
        return pltpu.make_async_remote_copy(
            sums.at[FAR, half_rows(h)], far.at[h], fsend.at[h], frecv.at[h],
            device_id={"tp": at_chip(x + chips - 1 if h else x + 1)}, device_id_type=MESH,
        )

    def near_copy(which, h):
        k = which - RIGHT
        return pltpu.make_async_remote_copy(
            sums.at[which, half_rows(h)], near.at[k, half_rows(h)], rsend.at[k, h], rrecv.at[k, h],
            device_id={"tp": at_chip(owner_of[which])}, device_id_type=MESH,
        )

    down(FAR, 0)
    far_copy(0).start()
    down(FAR, 1)
    far_copy(1).start()
    down(RIGHT, 1)
    near_copy(RIGHT, 1).start()
    down(LEFT, 0)
    near_copy(LEFT, 0).start()
    down(OWN, 0)
    far_copy(0).wait_recv()
    down(RIGHT, 0, 0)
    near_copy(RIGHT, 0).start()
    far_copy(1).wait_recv()
    down(LEFT, 1, 1)
    near_copy(LEFT, 1).start()
    down(OWN, 1)

    def total_rows(h):
        def body(i, _):
            r = pl.ds(pl.multiple_of(h * side_rows + i * tile, tile), tile)
            v = res[me, r, :].astype(F32) + sums[OWN, r, :].astype(F32)
            for k in range(2):
                v = v + near[k, r, :].astype(F32)
            out_ref[r, :] = v.astype(BF16)
            return 0

        lax.fori_loop(0, side_rows // tile, body, 0)

    for which, h in ((RIGHT, 1), (LEFT, 0), (RIGHT, 0), (LEFT, 1)):
        near_copy(which, h).wait_recv()
    for h in range(2):
        total_rows(h)

    for g in gathers:
        g.drain()
    for j in range(full + 1):
        for h in range(2):
            hcopy(h, j, core).wait_send()

    def outs_left(slot, _):
        @pl.when(lax.div(slot, per) != me)
        def _():
            ocopy(slot, me).wait_send()

        return 0

    lax.fori_loop(0, zn, outs_left, 0)
    each_arrival(lambda d, s: ycopy(d, s, side).wait_send(), own=False)
    for off in BEHIND:
        across(off, side).wait_send()
    for off in ROUTE:
        acopy(off, True).wait_send()
    for k in range(2):
        opposite(k, True).wait_send()
    for b in range(2):
        each_arrival(lambda d, s, b=b: hand(b, d, s, core).wait_send())
    for h in range(2):
        far_copy(h).wait_send()
        near_copy(RIGHT, h).wait_send()
        near_copy(LEFT, h).wait_send()


def layer(gn, zn, tn, tokens, mix_gain, in_m, in_s, pool_m, pool_s, out_m, out_s, ffn_gain,
          gate_m, gate_s, up_m, up_s, gate_t, up_t, down_m, down_s):
    _, length, width = tokens.shape
    depth, chan = in_m.shape
    ff = gate_m.shape[1]
    ocols = out_m.shape[1]
    per = width // ocols
    assert ff % LANES == LANES // 2 and per == 2 and chan == LANES and tn == 4 * CORES and gn % 2 == 0 and zn == 2 * OPPOSITE
    tiles = ff // LANES + 1
    hops = zn // 2
    dma = pltpu.SemaphoreType.DMA
    vmem = pl.BlockSpec(memory_space=pltpu.VMEM)
    out = pl.pallas_call(
        functools.partial(kernel, zn, tn),
        out_shape=jax.ShapeDtypeStruct((length, width), BF16),
        in_specs=[pl.BlockSpec(memory_space=pl.ANY)] + [vmem] * 16,
        out_specs=vmem,
        scratch_shapes=[
            pltpu.VMEM((tn, length, width), BF16),
            pltpu.VMEM((tn, length, width), BF16),
            pltpu.VMEM((length, tn * width), BF16),
            pltpu.VMEM((zn, 2, depth, chan), BF16),
            pltpu.VMEM((zn * depth, chan), BF16),
            pltpu.VMEM((tn, per, 2, chan // 2, ocols), BF16),
            pltpu.VMEM((tn * chan, width), BF16),
            pltpu.VMEM((length, chan), F32),
            pltpu.VMEM((tn, length, chan), BF16),
            pltpu.VMEM((zn * depth, 2 * ff), BF16),
            pltpu.VMEM((8, 2 * ff), F32),
            pltpu.VMEM((length // 2 + 8, 2 * LANES), F32),
            pltpu.VMEM((tiles, 8, 2 * LANES), F32),
            pltpu.VMEM((CORES, tiles, length, LANES), BF16),
            pltpu.VMEM((CORES, zn, tiles * LANES, ocols), BF16),
            pltpu.VMEM((4, length, width), BF16),
            pltpu.VMEM((2, length // 2, width), BF16),
            pltpu.VMEM((2, length, width), BF16),
            dma,
            dma((4, 2)), dma((4, 2, hops)),
            dma((4, FeatureGather.TAGS)), dma((4, FeatureGather.TAGS)),
            dma((zn,)), dma((tn, per)),
            dma((2, tiles)), dma((2, tiles)),
            dma((2, 2, hops + 1)), dma((2, 2, hops + 1)),
            dma((2, hops + 1)), dma((2, hops + 1)),
            dma((zn,)), dma((zn,)), dma((2,)), dma((2,)), dma((zn,)), dma((zn,)),
            dma((2,)), dma((2,)),
            dma((2, 2)), dma((2, 2)),
        ],
        compiler_params=pltpu.CompilerParams(
            collective_id=0, has_side_effects=True, vmem_limit_bytes=66_000_000
        ),
    )(
        tokens.reshape(length, width), mix_gain.reshape(1, -1), in_m, in_s, pool_m, pool_s, out_m, out_s,
        ffn_gain.reshape(1, -1), gate_m.T, gate_s, up_m.T, up_s, gate_t, up_t, down_m, down_s,
    )
    return out.reshape(tokens.shape)


def solution(mesh):
    return jax.shard_map(
        functools.partial(layer, mesh.shape["grp"], mesh.shape["fs"], mesh.shape["tp"]),
        mesh=mesh,
        in_specs=(
            P(("grp", "fs"), None, "tp"),
            P(),
            P("fs", "tp"),
            P(None, "tp"),
            P("tp", None, None),
            P(None, "tp"),
            P("tp", "fs"),
            P(None, "fs"),
            P(),
            P("fs", "tp"),
            P(None, "tp"),
            P("fs", "tp"),
            P(None, "tp"),
            P(None, "tp"),
            P(None, "tp"),
            P("tp", "fs"),
            P(None, "fs"),
        ),
        out_specs=P(("grp", "fs"), None, "tp"),
        check_vma=False,
    )
```

```python
import functools

import jax
import jax.numpy as jnp
from jax import lax
from jax.experimental import pallas as pl
from jax.experimental.pallas import tpu as pltpu
from jax.sharding import PartitionSpec as P

MESH = pl.DeviceIdType.MESH
EPS = 1e-06
BF16 = jnp.bfloat16
F32 = jnp.float32
LANES = 128
CORES = 2
ROUTE = {
    1: (0, 1), 15: (0, -1), 2: (0, 2), 14: (0, -2), 4: (0, 4), 12: (0, -4),
    5: (4, 1), 3: (4, -1), 6: (4, 2), 13: (12, 1), 11: (12, -1), 10: (12, -2), 9: (8, 1), 7: (8, -1),
}
QUARTER, OPPOSITE = 4, 8
BEHIND = (*ROUTE, OPPOSITE)


class FeatureGather:
    TAGS = 13
    R0, R1, L1, L0, F0, F1, OWN, PL0, PL1, PR0, PR1, PO0, PO1 = range(13)

    def __init__(self, buf, send, recv, chips, x, core, base, count):
        self.buf, self.send, self.recv = buf, send, recv
        self.base, self.half = base, count // 2
        at = lambda chip, c: lax.rem(chip, chips) * CORES + c
        other = 1 - core
        self.me, self.mate = at(x, core), at(x, other)
        self.right, self.left, self.far = at(x + 1, core), at(x + chips - 1, core), at(x + 2, core)
        mright, mleft, mfar = at(x + 1, other), at(x + chips - 1, other), at(x + 2, other)
        self.out = {
            self.R0: (self.me, 0, self.right), self.R1: (self.me, 1, self.right),
            self.L1: (self.me, 1, self.left), self.L0: (self.me, 0, self.left),
            self.F0: (self.left, 0, self.right), self.F1: (self.right, 1, self.left),
            self.OWN: (self.me, None, self.mate),
            self.PL0: (self.left, 0, self.mate), self.PL1: (self.left, 1, self.mate),
            self.PR0: (self.right, 0, self.mate), self.PR1: (self.right, 1, self.mate),
            self.PO0: (self.far, 0, self.mate), self.PO1: (self.far, 1, self.mate),
        }
        self.inn = {
            self.R0: (self.left, 0), self.R1: (self.left, 1),
            self.L1: (self.right, 1), self.L0: (self.right, 0),
            self.F0: (self.far, 0), self.F1: (self.far, 1),
            self.OWN: (self.mate, None),
            self.PL0: (mleft, 0), self.PL1: (mleft, 1),
            self.PR0: (mright, 0), self.PR1: (mright, 1),
            self.PO0: (mfar, 0), self.PO1: (mfar, 1),
        }
        self.then = {
            self.R0: (self.F0, self.PL0), self.L1: (self.F1, self.PR1),
            self.R1: (self.PL1,), self.L0: (self.PR0,),
            self.F0: (self.PO0,), self.F1: (self.PO1,),
        }

    def ref(self, block, part):
        if part is None:
            return self.buf.at[block, pl.ds(self.base, 2 * self.half)]
        return self.buf.at[block, pl.ds(self.base + part * self.half, self.half)]

    def copy(self, tag, block, part, to):
        ref = self.ref(block, part)
        return pltpu.make_async_remote_copy(
            ref, ref, self.send.at[tag], self.recv.at[tag], device_id={"tp": to}, device_id_type=MESH
        )

    def start(self):
        for tag in (self.R0, self.L1, self.R1, self.L0, self.OWN):
            self.copy(tag, *self.out[tag]).start()

    def arrive(self, *tags):
        for tag in tags:
            self.copy(tag, *self.inn[tag], self.mate).wait_recv()
            for later in self.then.get(tag, ()):
                self.copy(later, *self.out[later]).start()

    def finish(self):
        self.arrive(self.OWN, self.PL0, self.PR1, self.PL1, self.PR0, self.PO0, self.PO1)

    def drain(self):
        for tag in range(self.TAGS):
            self.copy(tag, *self.out[tag]).wait_send()


def down_cuts(ff):
    n = (ff // 3 + 31) // 32 * 32
    return (0, n), (n, n), (2 * n, ff - 2 * n)


def kernel(
    zn, tn,
    tok_in, mix_gain, in_m, in_s, pool_m, pool_s, out_m, out_s, ffn_gain,
    gate_m, gate_s, up_m, up_s, gate_t, up_t, down_m, down_s,
    out_ref,
    tok, res, nf, io, inw, outg, outw, proj, pool, gu, par, lin, edge, hid, dn, sums, far, near,
    load_sem, zsend, zrecv, gsend, grecv, osend, orecv, hsend, hrecv, dsend, drecv,
    ysend, yrecv, asend, arecv, esend, erecv, xsend, xrecv, fsend, frecv, rsend, rrecv,
):
    z, me, group = lax.axis_index("fs"), lax.axis_index("tp"), lax.axis_index("grp")
    side = lax.rem(group, 2)
    twin = group + 1 - 2 * side
    x, core = lax.div(me, CORES), lax.rem(me, CORES)
    other = 1 - core
    mate = x * CORES + other
    chips = tn // CORES
    zright, zleft = lax.rem(z + 1, zn), lax.rem(z + zn - 1, zn)
    hops = zn // 2

    length, width = tok_in.shape
    depth, chan = in_m.shape
    ff = gate_m.shape[0]
    ocols = out_m.shape[1]
    full = ff // LANES
    tail = ff - full * LANES
    per = width // ocols

    barrier = pltpu.get_barrier_semaphore()
    reach = sorted({o for _, o in ROUTE.values()})
    for o in reach:
        pl.semaphore_signal(barrier, inc=1, device_id={"fs": lax.rem(z + o + zn, zn)}, device_id_type=MESH)
    for j in range(1, tn):
        pl.semaphore_signal(barrier, inc=1, device_id={"tp": lax.rem(me + j, tn)}, device_id_type=MESH)
    pl.semaphore_signal(barrier, inc=1, device_id={"grp": twin}, device_id_type=MESH)

    load = pltpu.make_async_copy(tok_in, tok.at[me], load_sem)
    load.start()

    half = depth // 2
    scaled_out = (out_m[...] * out_s[...]).astype(BF16)
    for k in range(2):
        io[z, k, 0:half, :] = in_m[k * half : (k + 1) * half, :].astype(BF16)
        io[z, k, half:, :] = scaled_out[k * half : (k + 1) * half]

    def packed(g_ref, u_ref):
        for j in range(full):
            cols = slice(j * LANES, (j + 1) * LANES)
            yield 2 * j * LANES, jnp.concatenate([g_ref[:, cols], u_ref[:, cols]], axis=1)
        yield 2 * full * LANES, jnp.concatenate([g_ref[:, full * LANES :], u_ref[:, full * LANES :]], axis=1)

    own_rows = pl.ds(pl.multiple_of(z * depth, depth), depth)
    for j in range(full):
        for k, ref in enumerate((gate_m, up_m)):
            at = (2 * j + k) * LANES
            gu[own_rows, at : at + LANES] = ref[j * LANES : (j + 1) * LANES, :].T.astype(BF16)
    rest = jnp.concatenate([gate_m[full * LANES :, :], up_m[full * LANES :, :]], axis=0)
    gu[own_rows, 2 * full * LANES :] = rest.T.astype(BF16)
    for at, v in packed(gate_s, up_s):
        par[0:1, at : at + v.shape[1]] = v
    for at, v in packed(gate_t, up_t):
        par[1:4, at : at + v.shape[1]] = v
    dn[core, z, 0:ff, :] = (down_m[...] * down_s[...]).astype(BF16)
    dpad = dn.shape[2]

    def clear(i, _):
        dn[0, i, ff:dpad, :] = jnp.zeros((dpad - ff, ocols), BF16)
        dn[1, i, ff:dpad, :] = jnp.zeros((dpad - ff, ocols), BF16)
        return 0

    lax.fori_loop(0, zn, clear, 0)
    edge[...] = jnp.zeros(edge.shape, F32)
    load.wait()

    pl.semaphore_wait(barrier, tn + len(reach))

    shared = 3 * depth // 8
    common = depth - 2 * shared

    def gu_ref(slot, a, m):
        return gu.at[pl.ds(pl.multiple_of(slot * depth + a, 16), m)]

    def gu_shared(slot, part, whose):
        n = 2 * shared // 3
        a, m = ((0, shared), (0, n), (n, shared - n))[0 if part is None else part + 1]
        return gu_ref(slot, whose * shared + a, m)

    def gu_common(slot, part):
        a, m = (0, common) if part is None else (part * (common // 2), common // 2)
        return gu_ref(slot, 2 * shared + a, m)

    def dn_part(r0, n):
        def at(slot, part):
            a, m = (r0, n) if part is None else (r0 + part * (n // 2), n // 2)
            return dn.at[core, slot, pl.ds(a, m)]

        return at

    lanes = [
        lambda slot, part: gu_shared(slot, part, side), gu_common,
        *(dn_part(*c) for c in down_cuts(ff)),
    ]
    B1, B2, *C = range(len(lanes))

    def zslot(d, s):
        return lax.rem(z + zn + (s if d else -s), zn)

    def zcopy(i, d, s, part, slot):
        ref = lanes[i](slot, part)
        return pltpu.make_async_remote_copy(
            ref, ref, zsend.at[i, d], zrecv.at[i, d, s - 1],
            device_id={"fs": zleft if d else zright}, device_id_type=MESH,
        )

    def zput(i, d, s, part=None):
        return zcopy(i, d, s, part, zslot(d, s - 1))

    def zgot(i, d, s, part=None):
        zcopy(i, d, s, part, zslot(d, s)).wait_recv()

    def zopen(i):
        for d in range(2):
            zput(i, d, 1).start()

    def tick(i, s):
        for d in range(2):
            static = isinstance(s, int)
            part = d if static and s == hops else None
            zgot(i, d, s, part)
            zput(i, d, s, part).wait_send()
            if not static or s < hops - 1:
                zput(i, d, s + 1).start()
            elif s == hops - 1:
                zput(i, d, s + 1, d).start()
            if not static or s < hops:
                handed(i, d, s)
        if isinstance(s, int) and s == hops:
            handed(i, 0, s)

    def ycopy(d, s, whose):
        ref = gu_shared(zslot(d, s), None, whose)
        return pltpu.make_async_remote_copy(
            ref, ref, ysend.at[d, s], yrecv.at[d, s], device_id={"grp": twin}, device_id_type=MESH
        )

    def hand(c, d, s, which):
        ref = dn.at[which, zslot(d, s), pl.ds(*down_cuts(ff)[c])]
        return pltpu.make_async_remote_copy(
            ref, ref, dsend.at[c, d, s], drecv.at[c, d, s], device_id={"tp": mate}, device_id_type=MESH
        )

    def ocopy(slot, src):
        owner = lax.div(slot, per)
        return pltpu.make_async_remote_copy(
            io.at[slot, pl.ds(0, 2), pl.ds(half, half)], outg.at[src, lax.rem(slot, per)],
            osend.at[slot], orecv.at[src, lax.rem(slot, per)],
            device_id={"tp": owner}, device_id_type=MESH,
        )

    def handed(i, d, s):
        if i == B1:
            if not (isinstance(s, int) and s == 1):
                ycopy(d, s, side).start()
        elif i in C:
            hand(i - C[0], d, s, core).start()

    def acopy(off, sending):
        behind, o = ROUTE[off]
        slot = lax.rem(z - (behind if sending else off) + zn, zn)
        ref = io.at[slot, side]
        return pltpu.make_async_remote_copy(
            ref, ref, asend.at[off], arecv.at[off],
            device_id={"fs": lax.rem(z + o + zn, zn)}, device_id_type=MESH,
        )

    def across(off, whose):
        ref = io.at[lax.rem(z - off + zn, zn), whose]
        return pltpu.make_async_remote_copy(
            ref, ref, xsend.at[off], xrecv.at[off], device_id={"grp": twin}, device_id_type=MESH
        )

    def aput(behind):
        for off, (b, _) in sorted(ROUTE.items(), key=lambda r: r[0] not in (QUARTER, -QUARTER % zn)):
            if b == behind:
                acopy(off, True).start()

    def agot(*offs):
        for off in offs:
            acopy(off, False).wait_recv()
            if off in (QUARTER, -QUARTER % zn):
                opposite(int(off != QUARTER), True).start()
                aput(off)
            across(off, side).start()

    def opposite(k, sending):
        o = -QUARTER if k else QUARTER
        slot = lax.rem(z + (-o if sending else OPPOSITE) + zn, zn)
        ref = io.at[slot, side, pl.ds(k * half, half)]
        return pltpu.make_async_remote_copy(
            ref, ref, esend.at[k], erecv.at[k],
            device_id={"fs": lax.rem(z + o + zn, zn)}, device_id_type=MESH,
        )

    def opposite_got():
        for k in range(2):
            opposite(k, False).wait_recv()
        aput(OPPOSITE)
        across(OPPOSITE, side).start()

    def a_all():
        for off in BEHIND:
            across(off, 1 - side).wait_recv()

        def body(slot, _):
            @pl.when(lax.div(slot, per) != me)
            def _():
                ocopy(slot, me).start()

            return 0

        lax.fori_loop(0, zn, body, 0)

    def each_arrival(fn, own=True):
        if own:
            fn(0, 0)

        def body(s, _):
            fn(0, s)
            fn(1, s)
            return 0

        lax.fori_loop(1, hops, body, 0)
        fn(0, hops)

    def steps():
        for s in range(1, hops + 1):
            tick(B1, s)
            if s == hops - 1:
                zopen(C[0])
            tick(B2, s)
            if s == hops - 1:
                for i in C[1:]:
                    zopen(i)
            yield
        for s in range(1, hops + 1):
            all_down(s)
            yield

    def all_down(s):
        for i in C:
            tick(i, s)

    ring = steps()

    def go(n):
        for _ in range(n):
            next(ring)

    gathers = [
        FeatureGather(buf, gsend.at[k], grecv.at[k], chips, x, core, base, count)
        for k, (buf, base, count) in enumerate(
            ((tok, 0, length), (pool, 0, length), (res, 0, length // 2), (res, length // 2, length // 2))
        )
    ]
    g_tok, g_pool, g_first, g_second = gathers
    G = FeatureGather

    aput(0)
    zopen(B1)
    zopen(B2)
    g_tok.start()
    for i in C:
        handed(i, 0, 0)

    def norm(buf, gain_ref, lo, hi):
        rows = 32

        def body(i, _):
            r = pl.ds(pl.multiple_of(i * rows, rows), rows)
            total = jnp.zeros((rows, width), F32)
            for p in range(tn):
                v = buf[p, r, :].astype(F32)
                total = total + v * v
            mean = jnp.sum(total, axis=1, keepdims=True) * (1.0 / (tn * width))
            scale = lax.rsqrt(mean + EPS)
            for p in range(tn):
                cols = slice(p * width, (p + 1) * width)
                nf[r, cols] = (buf[p, r, :].astype(F32) * scale * gain_ref[:, cols]).astype(BF16)
            return 0

        lax.fori_loop(lo // rows, hi // rows, body, 0)

    agot(4, 12)
    agot(1, 15, 2, 14)
    g_tok.arrive(G.R0, G.L1)
    opposite_got()
    go(1)
    agot(5, 3, 6, 13, 11, 10)
    agot(9, 7)
    for d in range(2):
        ycopy(d, 1, side).start()
    g_tok.arrive(G.R1, G.L0)
    go(1)
    a_all()
    g_tok.arrive(G.F0, G.F1)
    g_tok.finish()
    part = length // 4
    norm(tok, mix_gain, 0, part)
    norm(tok, mix_gain, part, 2 * part)
    go(1)
    norm(tok, mix_gain, 2 * part, 3 * part)
    norm(tok, mix_gain, 3 * part, length)

    for k in range(zn):
        for h in range(2):
            inw[k * depth + h * half : k * depth + (h + 1) * half, :] = io[k, h, 0:half, :]
    tile = length // 4

    def project(i, _):
        r = pl.ds(pl.multiple_of(i * tile, tile), tile)
        v = jnp.dot(nf[r, :], inw[...], preferred_element_type=F32) * in_s[...]
        proj[r, :] = v.astype(BF16).astype(F32)
        return 0

    lax.fori_loop(0, 4, project, 0)

    v = proj[...]
    row = lax.broadcasted_iota(jnp.int32, v.shape, 0)

    def back(a, k):
        return jnp.where(row >= k, pltpu.roll(a, k, 0), 0.0)

    s2 = v + back(v, 1)
    s4 = s2 + back(s2, 2)
    s8 = s4 + back(s4, 4)
    s16 = s8 + back(s8, 8)
    total = jnp.where(x == 0, s2, jnp.where(x == 1, s4, jnp.where(x == 2, s8, s16)))
    count = jnp.minimum(row + 1, lax.shift_left(jnp.int32(2), x)).astype(F32)
    spread = (total / count - v).astype(BF16)
    mixed = jnp.dot(spread, pool_m[0], preferred_element_type=F32) * pool_s[...]
    pool[me] = mixed.astype(BF16)
    g_pool.start()

    go(1)
    g_pool.arrive(G.R0, G.L1)

    def others(fn):
        for j in range(1, tn):
            for k in range(per):
                fn(lax.rem(me + j, tn), k)

    others(lambda p, k: ocopy(me * per + k, p).wait_recv())
    for k in range(per):
        outg[me, k] = io[me * per + k, :, half:, :]
    for p in range(tn):
        for k in range(per):
            for h in range(2):
                rows = slice(p * chan + h * half, p * chan + (h + 1) * half)
                outw[rows, k * ocols : (k + 1) * ocols] = outg[p, k, h]
    go(1)
    g_pool.arrive(G.R1, G.L0)
    g_pool.arrive(G.F0, G.F1)
    g_pool.finish()

    def mix(i, _):
        r = pl.ds(pl.multiple_of(i * tile, tile), tile)
        rows = jnp.concatenate([pool[p, r, :] for p in range(tn)], axis=1)
        v = jnp.dot(rows, outw[...], preferred_element_type=F32)
        res[me, r, :] = (tok[me, r, :].astype(F32) + v).astype(BF16)
        return 0

    lax.fori_loop(0, 2, mix, 0)
    g_first.start()
    lax.fori_loop(2, 4, mix, 0)
    go(2)
    g_first.arrive(G.R0, G.L1)
    g_second.start()
    go(1)
    g_first.arrive(G.R1, G.L0)
    g_first.arrive(G.F0, G.F1)
    go(1)
    g_first.finish()
    norm(res, ffn_gain, 0, length // 2)

    g_second.arrive(G.R0, G.L1)
    all_down(2)
    each_arrival(lambda d, s: ycopy(d, s, 1 - side).wait_recv(), own=False)

    side_rows = length // 2
    taps = lin.shape[0] - side_rows

    def tile_product(h, j, at, n):
        lin[0:taps, 0:n] = edge[j, :, 0:n]

        def body(i, _):
            r = pl.ds(pl.multiple_of(h * side_rows + i * tile, tile), tile)
            v = jnp.dot(nf[r, :], gu[:, pl.ds(at, n)], preferred_element_type=F32)
            v = (v * par[0:1, pl.ds(at, n)]).astype(BF16).astype(F32)
            lin[pl.ds(pl.multiple_of(taps + i * tile, 8), tile), 0:n] = v
            return 0

        lax.fori_loop(0, side_rows // tile, body, 0)
        edge[j, :, 0:n] = lin[side_rows:, 0:n]

    chunk = 64

    def convolved(i, at, off):
        w = lin[pl.ds(pl.multiple_of(i * chunk, 8), chunk + taps), off : off + LANES]
        t = par[:, pl.ds(at + off, LANES)]
        return (
            t[3:4] * w[taps:] + t[2:3] * pltpu.roll(w, 1, 0)[taps:] + t[1:2] * pltpu.roll(w, 2, 0)[taps:]
        )

    def silu(g):
        return g / (1.0 + jnp.exp(-g))

    def hcopy(h, j, which):
        ref = hid.at[which, j, pl.ds(h * side_rows, side_rows)]
        return pltpu.make_async_remote_copy(
            ref, ref, hsend.at[h, j], hrecv.at[h, j], device_id={"tp": mate}, device_id_type=MESH
        )

    def store_rows(h, i):
        return pl.ds(pl.multiple_of(h * side_rows + i * chunk, chunk), chunk)

    def column(h, j):
        at = pl.multiple_of(j * 2 * LANES, 2 * LANES)
        tile_product(h, j, at, 2 * LANES)

        def body(i, _):
            v = silu(convolved(i, at, 0)) * convolved(i, at, LANES)
            hid[core, j, store_rows(h, i), :] = v.astype(BF16)
            return 0

        lax.fori_loop(0, side_rows // chunk, body, 0)
        hcopy(h, j, core).start()

    last = 2 * full * LANES
    lane = lax.broadcasted_iota(jnp.int32, (chunk, LANES), 1)

    def narrow_column(h):
        tile_product(h, full, last, LANES)

        def body(i, _):
            y = convolved(i, last, 0)
            v = jnp.where(lane < tail, silu(y) * pltpu.roll(y, LANES - tail, 1), 0.0)
            hid[core, full, store_rows(h, i), :] = v.astype(BF16)
            return 0

        lax.fori_loop(0, side_rows // chunk, body, 0)
        hcopy(h, full, core).start()

    def feed(h, after):
        def body(j, _):
            column(h, j)
            after(j)
            return 0

        lax.fori_loop(0, full, body, 0)
        narrow_column(h)

    def one_lane(j, start):
        for k in range(full):

            @pl.when(j == k)
            def _(k=k):
                tick(C[(start + k) % len(C)], (start + k) // len(C))

    def after_first(j):
        @pl.when(j == 0)
        def _():
            g_second.arrive(G.R1, G.L0)

        @pl.when(j == 2)
        def _():
            g_second.arrive(G.F0, G.F1)

        one_lane(j, 3 * len(C) + 1)

    def after_second(j):
        one_lane(j, 6 * len(C) + 1)

    tick(C[0], 3)
    feed(0, after_first)
    tick(C[0], 5)
    g_second.finish()
    tick(C[1], 5)
    norm(res, ffn_gain, side_rows, side_rows + side_rows // 2)
    tick(C[2], 5)
    norm(res, ffn_gain, side_rows + side_rows // 2, length)
    tick(C[0], 6)
    feed(1, after_second)
    all_down(hops)

    for j in range(full + 1):
        for h in range(2):
            hcopy(h, j, other).wait_recv()
    for c in range(len(C)):
        each_arrival(lambda d, s, c=c: hand(c, d, s, other).wait_recv())

    at_chip = lambda m: lax.rem(m, chips) * CORES + core
    FAR, RIGHT, LEFT, OWN = range(4)
    owner_of = (x + 2, x + 1, x + chips - 1, x)

    def down(which, h, extra=None):
        m = lax.rem(owner_of[which], chips)
        slot = (m * CORES + core) * per

        def body(i, _):
            r = pl.ds(pl.multiple_of(h * side_rows + i * tile, tile), tile)
            rows = jnp.concatenate([hid[k, j, r, :] for k in range(CORES) for j in range(full + 1)], axis=1)
            cols = jnp.concatenate(
                [jnp.concatenate([dn[k, slot + p] for p in range(per)], axis=1) for k in range(CORES)], axis=0
            )
            v = jnp.dot(rows, cols, preferred_element_type=F32)
            if extra is not None:
                v = v + far[extra, pl.ds(pl.multiple_of(i * tile, tile), tile), :].astype(F32)
            sums[which, r, :] = v.astype(BF16)
            return 0

        lax.fori_loop(0, side_rows // tile, body, 0)

    def half_rows(h):
        return pl.ds(h * side_rows, side_rows)

    def far_copy(h):
        return pltpu.make_async_remote_copy(
            sums.at[FAR, half_rows(h)], far.at[h], fsend.at[h], frecv.at[h],
            device_id={"tp": at_chip(x + chips - 1 if h else x + 1)}, device_id_type=MESH,
        )

    def near_copy(which, h):
        k = which - RIGHT
        return pltpu.make_async_remote_copy(
            sums.at[which, half_rows(h)], near.at[k, half_rows(h)], rsend.at[k, h], rrecv.at[k, h],
            device_id={"tp": at_chip(owner_of[which])}, device_id_type=MESH,
        )

    down(FAR, 0)
    far_copy(0).start()
    down(FAR, 1)
    far_copy(1).start()
    down(RIGHT, 1)
    near_copy(RIGHT, 1).start()
    down(LEFT, 0)
    near_copy(LEFT, 0).start()
    down(OWN, 0)
    far_copy(0).wait_recv()
    down(RIGHT, 0, 0)
    near_copy(RIGHT, 0).start()
    far_copy(1).wait_recv()
    down(LEFT, 1, 1)
    near_copy(LEFT, 1).start()
    down(OWN, 1)

    def total_rows(h):
        def body(i, _):
            r = pl.ds(pl.multiple_of(h * side_rows + i * tile, tile), tile)
            v = res[me, r, :].astype(F32) + sums[OWN, r, :].astype(F32)
            for k in range(2):
                v = v + near[k, r, :].astype(F32)
            out_ref[r, :] = v.astype(BF16)
            return 0

        lax.fori_loop(0, side_rows // tile, body, 0)

    for which, h in ((RIGHT, 1), (LEFT, 0), (RIGHT, 0), (LEFT, 1)):
        near_copy(which, h).wait_recv()
    for h in range(2):
        total_rows(h)

    for g in gathers:
        g.drain()
    for j in range(full + 1):
        for h in range(2):
            hcopy(h, j, core).wait_send()

    def outs_left(slot, _):
        @pl.when(lax.div(slot, per) != me)
        def _():
            ocopy(slot, me).wait_send()

        return 0

    lax.fori_loop(0, zn, outs_left, 0)
    each_arrival(lambda d, s: ycopy(d, s, side).wait_send(), own=False)
    for off in BEHIND:
        across(off, side).wait_send()
    for off in ROUTE:
        acopy(off, True).wait_send()
    for k in range(2):
        opposite(k, True).wait_send()
    for c in range(len(C)):
        each_arrival(lambda d, s, c=c: hand(c, d, s, core).wait_send())
    for h in range(2):
        far_copy(h).wait_send()
        near_copy(RIGHT, h).wait_send()
        near_copy(LEFT, h).wait_send()


def layer(gn, zn, tn, tokens, mix_gain, in_m, in_s, pool_m, pool_s, out_m, out_s, ffn_gain,
          gate_m, gate_s, up_m, up_s, gate_t, up_t, down_m, down_s):
    _, length, width = tokens.shape
    depth, chan = in_m.shape
    ff = gate_m.shape[1]
    ocols = out_m.shape[1]
    per = width // ocols
    assert ff % LANES == LANES // 2 and per == 2 and chan == LANES and tn == 4 * CORES and gn % 2 == 0 and zn == 2 * OPPOSITE
    tiles = ff // LANES + 1
    hops = zn // 2
    dma = pltpu.SemaphoreType.DMA
    vmem = pl.BlockSpec(memory_space=pltpu.VMEM)
    out = pl.pallas_call(
        functools.partial(kernel, zn, tn),
        out_shape=jax.ShapeDtypeStruct((length, width), BF16),
        in_specs=[pl.BlockSpec(memory_space=pl.ANY)] + [vmem] * 16,
        out_specs=vmem,
        scratch_shapes=[
            pltpu.VMEM((tn, length, width), BF16),
            pltpu.VMEM((tn, length, width), BF16),
            pltpu.VMEM((length, tn * width), BF16),
            pltpu.VMEM((zn, 2, depth, chan), BF16),
            pltpu.VMEM((zn * depth, chan), BF16),
            pltpu.VMEM((tn, per, 2, chan // 2, ocols), BF16),
            pltpu.VMEM((tn * chan, width), BF16),
            pltpu.VMEM((length, chan), F32),
            pltpu.VMEM((tn, length, chan), BF16),
            pltpu.VMEM((zn * depth, 2 * ff), BF16),
            pltpu.VMEM((8, 2 * ff), F32),
            pltpu.VMEM((length // 2 + 8, 2 * LANES), F32),
            pltpu.VMEM((tiles, 8, 2 * LANES), F32),
            pltpu.VMEM((CORES, tiles, length, LANES), BF16),
            pltpu.VMEM((CORES, zn, tiles * LANES, ocols), BF16),
            pltpu.VMEM((4, length, width), BF16),
            pltpu.VMEM((2, length // 2, width), BF16),
            pltpu.VMEM((2, length, width), BF16),
            dma,
            dma((5, 2)), dma((5, 2, hops)),
            dma((4, FeatureGather.TAGS)), dma((4, FeatureGather.TAGS)),
            dma((zn,)), dma((tn, per)),
            dma((2, tiles)), dma((2, tiles)),
            dma((3, 2, hops + 1)), dma((3, 2, hops + 1)),
            dma((2, hops + 1)), dma((2, hops + 1)),
            dma((zn,)), dma((zn,)), dma((2,)), dma((2,)), dma((zn,)), dma((zn,)),
            dma((2,)), dma((2,)),
            dma((2, 2)), dma((2, 2)),
        ],
        compiler_params=pltpu.CompilerParams(
            collective_id=0, has_side_effects=True, vmem_limit_bytes=66_000_000
        ),
    )(
        tokens.reshape(length, width), mix_gain.reshape(1, -1), in_m, in_s, pool_m, pool_s, out_m, out_s,
        ffn_gain.reshape(1, -1), gate_m.T, gate_s, up_m.T, up_s, gate_t, up_t, down_m, down_s,
    )
    return out.reshape(tokens.shape)


def solution(mesh):
    return jax.shard_map(
        functools.partial(layer, mesh.shape["grp"], mesh.shape["fs"], mesh.shape["tp"]),
        mesh=mesh,
        in_specs=(
            P(("grp", "fs"), None, "tp"),
            P(),
            P("fs", "tp"),
            P(None, "tp"),
            P("tp", None, None),
            P(None, "tp"),
            P("tp", "fs"),
            P(None, "fs"),
            P(),
            P("fs", "tp"),
            P(None, "tp"),
            P("fs", "tp"),
            P(None, "tp"),
            P(None, "tp"),
            P(None, "tp"),
            P("tp", "fs"),
            P(None, "fs"),
        ),
        out_specs=P(("grp", "fs"), None, "tp"),
        check_vma=False,
    )
```
